256 devices in a mesh: sp: 64 (over z, x, core), tp: 4 (over y).
Axes of the slice: x: 4, y: 4, z: 8, core: 2. Of those that a mesh axis runs over, the one named last changes fastest.
Arguments:
- queries: bfloat16 [65536, 2048], P('sp', 'tp'), may hold values from -16 to 16
- key_rows: bfloat16 [65536, 512], P('sp', 'tp'), may hold values from -16 to 16
- value_rows: bfloat16 [65536, 512], P('sp', 'tp'), may hold values from -6 to 6
- doc_ids: int32 [65536], P('sp'), may hold values from 0 to 31, never falling along the last dimension, each value on 1 to 4096 neighbouring positions
- sink_logit: float32 [32], P('tp'), may hold values from 3 to 7
- residual: bfloat16 [65536, 2048], P(('sp', 'tp')), may hold values from -6 to 6
- out_weight: bfloat16 [2048, 2048], P('tp'), may hold values from -3.5 to 3.5
- norm_gain: float32 [2048], replicated, may hold values from 0.1 to 1.9
- gate_weight: bfloat16 [64, 2048, 512], P('sp'), may hold values from -0.125 to 0.125
- up_weight: bfloat16 [64, 2048, 512], P('sp'), may hold values from -0.125 to 0.125
- down_weight: bfloat16 [64, 512, 2048], P('sp'), may hold values from -0.25 to 0.25
- routes: int32 [65536, 2], P(('sp', 'tp')), may hold values from 0 to 63, as said below
- route_weights: float32 [65536, 2], P(('sp', 'tp')), may hold values from 0.2 to 0.8
Outputs:
- mixed: bfloat16 [65536, 2048], P(('sp', 'tp'))
The draws below stay inside these ranges and needn't reach their ends.
Inputs may be any that keep to these rules, and one draw needn't show every extreme that they name: `doc_ids`: never falls along the positions. `routes`: each aligned block of 256 rows names every expert exactly 8 times; the experts of one row differ and lie in one group of 16 consecutive numbers.
All inputs are finite; a program needn't handle non-finite values.
Results may differ from the reference program's by a relative error of at most 0.012.
Values may be sent and summed in bfloat16 or wider, within the bound.
A program may use at most 128 MiB of HBM per device.

```python
import math
import jax
import jax.numpy as jnp
import numpy as np
from jax import lax

D = 2048
HEADS = 32
KV_HEADS = 8
HD = 64
FF = 512
WINDOW = 128
GROUPS = 4
TOPK = 2
TOKENS = 65536
EXPERTS = 64
GROUP_SIZE = 16
ROWS_HOME = 256
CAP = 8
DOCS = 32
DOC_MOST = 4096
N_TP = 4


def draw_queries(key, part):
    noise = jax.random.truncated_normal(jax.random.fold_in(key, 11), -4.0, 4.0, (TOKENS, HEADS * HD), jnp.float32)
    return noise.astype(jnp.bfloat16)


def draw_key_rows(key, part):
    noise = jax.random.truncated_normal(jax.random.fold_in(key, 12), -4.0, 4.0, (TOKENS, KV_HEADS * HD), jnp.float32)
    return noise.astype(jnp.bfloat16)


def draw_routes(key, part):
    block_total = TOKENS // ROWS_HOME
    half_slots = GROUP_SIZE * CAP // 2

    def one_block(block_key):
        order_key, shuffle_key = jax.random.split(block_key)
        group_keys = jax.random.split(order_key, GROUPS)
        ordering = jax.vmap(lambda group_key: jax.random.permutation(group_key, GROUP_SIZE))(group_keys)
        ordering = ordering.astype(jnp.int32) + (jnp.arange(GROUPS, dtype=jnp.int32) * GROUP_SIZE)[:, None]
        slot_ids = jnp.arange(half_slots, dtype=jnp.int32)
        leading = ordering[:, slot_ids // CAP]
        trailing = ordering[:, (slot_ids + half_slots) // CAP]
        paired = jnp.stack([leading.reshape(-1), trailing.reshape(-1)], axis=1)
        shuffle = jax.random.permutation(shuffle_key, ROWS_HOME)
        return paired[shuffle].astype(jnp.int32)
    blocks = jax.vmap(one_block)(jax.random.split(jax.random.fold_in(key, 77), block_total))
    return blocks.reshape(TOKENS, TOPK)


def levels(key, shape, cuts, low, high):
    gain, own = 1.0, jax.random.fold_in(key, 6)
    for dim, blocks in cuts:
        draws = jnp.exp(jax.random.uniform(jax.random.fold_in(own, dim), (blocks,), jnp.float32, low / len(cuts), high / len(cuts)))
        gain = gain * jnp.repeat(draws, shape[dim] // blocks).reshape([-1 if axis == dim else 1 for axis in range(len(shape))])
    return gain


def split_up(number_of, total, limit, lean):
    portions = [(1 << 20) // math.isqrt(standing ** lean) + 1 for standing in range(2, number_of + 1)]
    rest, counts = total - limit - (number_of - 1), [1] * (number_of - 1)
    while rest > 0:
        candidates = [i for i in range(number_of - 1) if counts[i] < limit]
        whole, remaining = sum([portions[i] for i in candidates]), rest
        for i in candidates:
            extra = min(limit - counts[i], max(1, remaining * portions[i] // whole), rest)
            counts[i] = counts[i] + extra
            rest = rest - extra
    return np.array([limit] + counts)


def uneven(own_key, number_of, total, bound, skew):
    if number_of == 2:
        one = jax.random.randint(own_key, (), max(1, total - bound), min(bound, total - 1) + 1)
        return jnp.stack([one, total - one])
    lengths = jnp.asarray(split_up(number_of, total, bound, skew), jnp.int32)
    pairs = (number_of - 1) // 2
    giver, taker = lengths[1:1 + 2 * pairs:2], lengths[2:2 + 2 * pairs:2]
    margin = jnp.minimum(giver - 1, bound - taker)
    moved = jax.random.randint(jax.random.fold_in(own_key, 1), (pairs,), 0, 1 << 20) % (margin + 1)
    lengths = lengths.at[1:1 + 2 * pairs:2].set(giver - moved).at[2:2 + 2 * pairs:2].set(taker + moved)
    return lengths[jax.random.permutation(jax.random.fold_in(own_key, 2), number_of)]


def normal_values(key, extent, width, most, pieces=(), kind=jnp.bfloat16):
    factor_of = levels(key, extent, pieces, -0.22, 0.18) if pieces else 1.0
    values = jax.random.normal(key, extent, jnp.float32) * width * factor_of
    return jnp.minimum(jnp.maximum(values, -most), most).astype(kind)


def setup_inputs(seed: int = 0) -> dict:
    keys = jax.random.split(jax.random.key(seed), 14)
    queries = draw_queries(jax.random.fold_in(keys[13], 71), 0)
    key_rows = draw_key_rows(jax.random.fold_in(keys[13], 71), 0)
    value_rows = normal_values(keys[2], (TOKENS, KV_HEADS * HD), 1.0, 6.0, ((0, 64), (1, 4)))
    doc_ids = jnp.searchsorted(jnp.cumsum(uneven(keys[3], DOCS, TOKENS, DOC_MOST, 1)), jnp.arange(TOKENS), side="right").astype(jnp.int32)
    sink_logit = jnp.clip(3.0 + 4.0 * jax.random.uniform(keys[4], (HEADS,), jnp.float32) ** levels(keys[4], (HEADS,), ((0, 4),), -0.2, 0.2), 3.0, 7.0)
    residual = normal_values(keys[5], (TOKENS, D), 1.0, 6.0, ((0, 256),))
    out_weight = normal_values(keys[6], (HEADS * HD, D), ((HEADS * HD) ** -0.5 * 10), 3.5, ((0, 4),))
    norm_gain = jnp.clip(1.0 + 0.18 * jax.random.normal(keys[7], (D,), jnp.float32), 0.1, 1.9)
    gate_weight = normal_values(keys[8], (EXPERTS, D, FF), D ** -0.5, 0.125, ((0, 64),))
    up_weight = normal_values(keys[9], (EXPERTS, D, FF), D ** -0.5, 0.125, ((0, 64),))
    down_weight = normal_values(keys[10], (EXPERTS, FF, D), FF ** -0.5, 0.25, ((0, 64),))
    routes = draw_routes(jax.random.fold_in(keys[13], 71), 0)
    route_weights = jnp.clip(0.2 + 0.6 * jax.random.uniform(keys[12], (TOKENS, TOPK), jnp.float32) ** levels(keys[12], (TOKENS, TOPK), ((0, 256),), -0.2, 0.2), 0.2, 0.8)
    return dict(queries=queries, key_rows=key_rows, value_rows=value_rows, doc_ids=doc_ids, sink_logit=sink_logit, residual=residual, out_weight=out_weight, norm_gain=norm_gain, gate_weight=gate_weight, up_weight=up_weight, down_weight=down_weight, routes=routes, route_weights=route_weights)


neg_fill = -1e+30
eps_norm = 1e-06

def reference(queries, key_rows, value_rows, doc_ids, sink_logit, residual, out_weight, norm_gain, gate_weight, up_weight, down_weight, routes, route_weights):
    head_ratio = HEADS // KV_HEADS
    block_rows = 512
    block_total = TOKENS // block_rows
    key_pad = jnp.pad(key_rows, ((WINDOW, WINDOW), (0, 0)))
    value_pad = jnp.pad(value_rows, ((WINDOW, WINDOW), (0, 0)))
    doc_pad = jnp.pad(doc_ids, (WINDOW, WINDOW), constant_values=-1)
    sink_col = sink_logit.astype(jnp.float32).reshape(KV_HEADS, head_ratio)[:, :, None, None]

    def one_block(block_index):
        row_start = (block_index * block_rows).astype(jnp.int32)
        key_count = block_rows + 2 * WINDOW
        query_part = lax.dynamic_slice_in_dim(queries, row_start, block_rows, 0).astype(jnp.float32)
        query_part = query_part.reshape(block_rows, KV_HEADS, head_ratio, HD)
        key_part = lax.dynamic_slice_in_dim(key_pad, row_start, key_count, 0).astype(jnp.float32).reshape(key_count, KV_HEADS, HD)
        value_part = lax.dynamic_slice_in_dim(value_pad, row_start, key_count, 0).astype(jnp.float32).reshape(key_count, KV_HEADS, HD)
        query_docs = lax.dynamic_slice_in_dim(doc_ids, row_start, block_rows, 0)
        key_docs = lax.dynamic_slice_in_dim(doc_pad, row_start, key_count, 0)
        query_pos = row_start + jnp.arange(block_rows, dtype=jnp.int32)
        key_pos = row_start - WINDOW + jnp.arange(key_count, dtype=jnp.int32)
        allowed = (jnp.abs(query_pos[:, None] - key_pos[None, :]) <= WINDOW) & (query_docs[:, None] == key_docs[None, :])
        scores = jnp.einsum('qgrd,kgd->grqk', query_part, key_part) * HD ** (-0.5)
        masked = jnp.where(allowed[None, None], scores, neg_fill)
        row_top = jnp.maximum(lax.optimization_barrier(jnp.max(masked, axis=3, keepdims=True)), sink_col)
        exponent = jnp.where(allowed[None, None], jnp.exp(masked - row_top), 0.0)
        denominator = lax.optimization_barrier(jnp.sum(exponent, axis=3, keepdims=True)) + jnp.exp(sink_col - row_top)
        attn_weight = (exponent / denominator).astype(jnp.bfloat16)
        attended = jnp.einsum('grqk,kgd->qgrd', attn_weight.astype(jnp.float32), value_part)
        return attended.astype(jnp.bfloat16).reshape(block_rows, HEADS * HD)
    attended = lax.map(one_block, jnp.arange(block_total, dtype=jnp.int32)).reshape(TOKENS, HEADS * HD)
    group_cols = HEADS * HD // N_TP
    summed = jnp.zeros((TOKENS, D), jnp.float32)
    for group_index in range(N_TP):
        cols = attended[:, group_index * group_cols:(group_index + 1) * group_cols]
        rows_w = out_weight[group_index * group_cols:(group_index + 1) * group_cols]
        partial_value = jnp.dot(cols, rows_w, preferred_element_type=jnp.float32).astype(jnp.bfloat16)
        partial_value = lax.optimization_barrier(partial_value)
        summed = summed + partial_value.astype(jnp.float32)
    stream = (residual.astype(jnp.float32) + summed).astype(jnp.bfloat16)
    stream_f = stream.astype(jnp.float32)
    scale = lax.rsqrt(lax.optimization_barrier(jnp.mean(stream_f * stream_f, axis=1, keepdims=True)) + eps_norm)
    normed = (stream_f * scale * norm_gain.astype(jnp.float32)[None, :]).astype(jnp.bfloat16)
    flat_routes = routes.reshape(-1)
    flat_weights = route_weights.reshape(-1).astype(jnp.float32)
    per_expert = TOKENS * TOPK // EXPERTS

    def expert_step(accum, inputs):
        expert_id, gate_one, up_one, down_one = inputs
        found = jnp.nonzero(flat_routes == expert_id, size=per_expert)[0].astype(jnp.int32)
        token_index = found // TOPK
        rows = normed[token_index]
        gate_act = jnp.dot(rows, gate_one, preferred_element_type=jnp.float32)
        up_act = jnp.dot(rows, up_one, preferred_element_type=jnp.float32)
        hidden = (jax.nn.silu(gate_act) * up_act).astype(jnp.bfloat16)
        expert_out = jnp.dot(hidden, down_one, preferred_element_type=jnp.float32).astype(jnp.bfloat16)
        accum = accum.at[token_index].add(flat_weights[found][:, None] * expert_out.astype(jnp.float32))
        return (accum, None)
    accum0 = jnp.zeros((TOKENS, D), jnp.float32)
    accum, _ = lax.scan(expert_step, accum0, (jnp.arange(EXPERTS, dtype=jnp.int32), gate_weight, up_weight, down_weight))
    return (stream_f + accum).astype(jnp.bfloat16)
```

```python
import jax
import jax.numpy as jnp
from jax import lax
from jax.experimental import pallas as pl
from jax.experimental.pallas import tpu as pltpu
from jax.sharding import PartitionSpec as P

HD = 64
BLK = 128
MESH = pl.DeviceIdType.MESH
NEG = -1e30
EPS = 1e-06
BF = jnp.bfloat16
F32 = jnp.float32


def coords():
    s = lax.axis_index("sp")
    y = lax.axis_index("tp")
    c = lax.rem(s, 2)
    x = lax.rem(s // 2, 4)
    z = s // 8
    return s, y, z, x, c


def sp_of(z, x, c):
    return (z * 4 + x) * 2 + c


def front_kernel(
    q_ref, k_ref, v_ref, docs_ref, sink_ref, gain_ref, resid_hbm, w_hbm,
    stream_ref, normed_ref,
    k2, v2, dpad, khalo, vhalo, att, regr, wall, w_own, resid, acc, bias,
    send, recv, lsem,
):
    s, y, z, x, c = coords()
    xm, xp = lax.rem(x + 3, 4), lax.rem(x + 1, 4)
    xo = lax.rem(x + 2, 4)
    sp_next = (lax.rem(s + 1, 64), y)
    sp_prev = (lax.rem(s + 63, 64), y)
    sib = (sp_of(z, x, 1 - c), y)
    x_next = (sp_of(z, xp, c), y)
    x_prev = (sp_of(z, xm, c), y)
    tps = [None] + [(s, lax.rem(y + r, 4)) for r in (1, 2, 3)]

    def rc(src, dst, n, dev):
        return pltpu.make_async_remote_copy(
            src_ref=src, dst_ref=dst, send_sem=send.at[n], recv_sem=recv.at[n],
            device_id=dev, device_id_type=MESH,
        )

    started = []

    def go(src, dst, n, dev):
        d = rc(src, dst, n, dev)
        d.start()
        started.append(d)

    def got(dst, n):
        rc(dst, dst, n, sib).wait_recv()

    w_copy = pltpu.make_async_copy(w_hbm, w_own, lsem.at[0])
    r_copy = pltpu.make_async_copy(resid_hbm, resid, lsem.at[1])
    w_copy.start()
    r_copy.start()
    barrier = pltpu.get_barrier_semaphore()
    for dev in (sp_next, sp_prev, tps[1], tps[2], tps[3], x_next, x_prev):
        pl.semaphore_signal(barrier, inc=1, device_id=dev, device_id_type=MESH)
    pl.semaphore_wait(barrier, 7)

    go(k_ref.at[pl.ds(896, 128)], khalo.at[0], 0, sp_next)
    go(v_ref.at[pl.ds(896, 128)], vhalo.at[0], 1, sp_next)
    go(docs_ref.at[7], dpad.at[0], 2, sp_next)
    go(k_ref.at[pl.ds(0, 128)], khalo.at[1], 3, sp_prev)
    go(v_ref.at[pl.ds(0, 128)], vhalo.at[1], 4, sp_prev)
    go(docs_ref.at[0], dpad.at[9], 5, sp_prev)

    def rows(xx, cc, off, n):
        return pl.ds(pl.multiple_of(128 * xx + 64 * cc + off, 32), n)

    w_copy.wait()
    mine = rows(x, c, 0, 64)
    mine_lo, mine_hi = rows(x, c, 0, 32), rows(x, c, 32, 32)
    go(w_own.at[mine], wall.at[0, mine], 6, tps[1])
    go(w_own.at[mine], wall.at[1, mine], 7, tps[3])

    lane = lax.broadcasted_iota(jnp.int32, (BLK, BLK), 1)
    row = lax.broadcasted_iota(jnp.int32, (BLK, BLK), 0)
    low = lane < 64

    def dup(src, dst, at):
        v = src.astype(F32)
        rolled = pltpu.roll(v, 64, 1)
        dst[0, pl.ds(at, BLK), :] = jnp.where(low, v, rolled).astype(BF)
        dst[1, pl.ds(at, BLK), :] = jnp.where(low, rolled, v).astype(BF)

    @pl.loop(0, 8)
    def _(i):
        at = pl.multiple_of(i * BLK, BLK)
        dup(k_ref[pl.ds(at, BLK), :], k2, at + BLK)
        dup(v_ref[pl.ds(at, BLK), :], v2, at + BLK)
        dpad[i + 1] = docs_ref[i]

    for n, ref in ((0, khalo.at[0]), (1, vhalo.at[0]), (2, dpad.at[0]),
                   (3, khalo.at[1]), (4, vhalo.at[1]), (5, dpad.at[9])):
        got(ref, n)
    dup(khalo[0], k2, 0)
    dup(khalo[1], k2, 9 * BLK)
    dup(vhalo[0], v2, 0)
    dup(vhalo[1], v2, 9 * BLK)
    dpad[0] = jnp.where(s == 0, -1, dpad[0])
    dpad[9] = jnp.where(s == 63, -1, dpad[9])

    scale = HD ** (-0.5)
    mrow = lax.broadcasted_iota(jnp.int32, (BLK, BLK), 1)
    m_even = jnp.where(mrow < 64, scale, 0.0).astype(BF)
    m_odd = jnp.where(mrow < 64, 0.0, scale).astype(BF)

    def pair_of_blocks(t, out, out_at):
        p = lax.rem(y + 1 + t, 4)

        @pl.loop(0, 4)
        def _(it):
            sub = it // 2
            g = lax.rem(it, 2)
            b = 2 * p + sub
            at = pl.multiple_of(b * BLK, BLK)

            @pl.when(g == 0)
            def _():
                qd = jnp.transpose(jnp.broadcast_to(dpad[b + 1].astype(F32), (BLK, BLK)))
                for j in range(3):
                    ok = qd == dpad[b + j].astype(F32)
                    if j == 0:
                        ok = ok & (lane >= row)
                    if j == 2:
                        ok = ok & (lane <= row)
                    bias[:, j * BLK:(j + 1) * BLK] = jnp.where(ok, 0.0, NEG)

            keys = k2[g, pl.ds(at, 3 * BLK), :]
            vals = v2[g, pl.ds(at, 3 * BLK), :]
            for pair in range(2):
                col = pl.multiple_of(g * 256 + pair * BLK, BLK)
                qq = q_ref[pl.ds(at, BLK), pl.ds(col, BLK)]
                outs = []
                for half in range(2):
                    sink = sink_ref[g * 4 + pair * 2 + half]
                    qm = qq * (m_even if half == 0 else m_odd)
                    sc = lax.dot_general(qm, keys, (((1,), (1,)), ((), ())),
                                         preferred_element_type=F32) + bias[...]
                    top = jnp.maximum(jnp.max(sc, axis=1, keepdims=True), sink)
                    ex = jnp.exp(sc - top)
                    den = jnp.sum(ex, axis=1, keepdims=True) + jnp.exp(sink - top)
                    o = jnp.dot(ex.astype(BF), vals, preferred_element_type=F32)
                    outs.append(o * (1.0 / den))
                out[out_at, pl.ds(pl.multiple_of(sub * BLK, BLK), BLK), pl.ds(col, BLK)] = (
                    jnp.where(low, outs[0], outs[1]).astype(BF))

    def send_att(t):
        r = t + 1
        go(att.at[t], regr.at[4 - r], 26 + t, tps[r])

    ab, dd = pl.ds(0, 2), pl.ds(2, 1)
    pair_of_blocks(0, att, 0)
    got(wall.at[0, mine], 6)
    got(wall.at[1, mine], 7)
    go(wall.at[0, mine_lo], wall.at[2, mine_lo], 8, tps[1])
    go(wall.at[1, mine_hi], wall.at[2, mine_hi], 9, tps[3])
    go(wall.at[ab, mine], wall.at[ab, mine], 10, x_next)
    go(wall.at[ab, mine], wall.at[ab, mine], 11, x_prev)
    go(wall.at[ab, mine], wall.at[ab, mine], 18, sib)
    pair_of_blocks(1, att, 1)
    send_att(0)
    pair_of_blocks(2, att, 2)
    send_att(1)
    got(wall.at[2, mine_lo], 8)
    got(wall.at[2, mine_hi], 9)
    go(wall.at[dd, mine], wall.at[dd, mine], 12, x_next)
    go(wall.at[dd, mine], wall.at[dd, mine], 13, x_prev)
    go(wall.at[dd, mine], wall.at[dd, mine], 19, sib)
    pair_of_blocks(3, regr, 0)
    send_att(2)

    from_m, from_p = rows(xm, c, 0, 64), rows(xp, c, 0, 64)
    fm_lo, fp_hi = rows(xm, c, 0, 32), rows(xp, c, 32, 32)
    far, far_lo, far_hi = rows(xo, c, 0, 64), rows(xo, c, 0, 32), rows(xo, c, 32, 32)

    for sh, n, nd in ((ab, 10, 20), (dd, 12, 21)):
        got(wall.at[sh, from_m], n)
        got(wall.at[sh, from_p], n + 1)
        go(wall.at[sh, fm_lo], wall.at[sh, fm_lo], n + 4, x_next)
        go(wall.at[sh, fp_hi], wall.at[sh, fp_hi], n + 5, x_prev)
        go(wall.at[sh, from_m], wall.at[sh, from_m], nd, sib)
        go(wall.at[sh, from_p], wall.at[sh, from_p], nd + 2, sib)

    r_copy.wait()
    acc[...] = resid[...].astype(F32)

    def project(r, wref):
        @pl.loop(0, 4)
        def _(n):
            cols = pl.ds(pl.multiple_of(n * 512, 512), 512)
            part = jnp.dot(regr[r], wref[:, cols], preferred_element_type=F32)
            acc[:, cols] += part.astype(BF).astype(F32)

    project(0, w_own)
    for sh, n, nd in ((ab, 14, 24), (dd, 16, 25)):
        got(wall.at[sh, far_lo], n)
        got(wall.at[sh, far_hi], n + 1)
        go(wall.at[sh, far], wall.at[sh, far], nd, sib)
        for xx, m in ((x, nd - 6), (xm, nd - 4), (xp, nd - 2), (xo, nd)):
            sl = rows(xx, 1 - c, 0, 64)
            got(wall.at[sh, sl], m)
        if n == 14:
            got(regr.at[1], 26 + 2)
            project(1, wall.at[1])
            got(regr.at[3], 26)
            project(3, wall.at[0])
        else:
            got(regr.at[2], 26 + 1)
            project(2, wall.at[2])

    @pl.loop(0, 16)
    def _(i):
        rr = pl.ds(pl.multiple_of(i * 16, 16), 16)
        st = acc[rr, :].astype(BF)
        stream_ref[rr, :] = st
        sf = st.astype(F32)
        sc = lax.rsqrt(jnp.mean(sf * sf, axis=1, keepdims=True) + EPS)
        normed_ref[rr, :] = (sf * sc * gain_ref[...]).astype(BF)

    for d in started:
        d.wait_send()


def front(queries, key_rows, value_rows, doc_ids, sink_logit, residual, out_weight, norm_gain):
    vm = pl.BlockSpec(memory_space=pltpu.VMEM)
    anyspec = pl.BlockSpec(memory_space=pl.ANY)
    return pl.pallas_call(
        front_kernel,
        out_shape=(
            jax.ShapeDtypeStruct((256, 2048), BF),
            jax.ShapeDtypeStruct((256, 2048), BF),
        ),
        in_specs=[vm, vm, vm, vm, pl.BlockSpec(memory_space=pltpu.SMEM), vm, anyspec, anyspec],
        out_specs=(vm, vm),
        scratch_shapes=[
            pltpu.VMEM((2, 1280, 128), BF),
            pltpu.VMEM((2, 1280, 128), BF),
            pltpu.VMEM((10, 1, 128), jnp.int32),
            pltpu.VMEM((2, 128, 128), BF),
            pltpu.VMEM((2, 128, 128), BF),
            pltpu.VMEM((3, 256, 512), BF),
            pltpu.VMEM((4, 256, 512), BF),
            pltpu.VMEM((3, 512, 2048), BF),
            pltpu.VMEM((512, 2048), BF),
            pltpu.VMEM((256, 2048), BF),
            pltpu.VMEM((256, 2048), F32),
            pltpu.VMEM((128, 384), F32),
            pltpu.SemaphoreType.DMA((29,)),
            pltpu.SemaphoreType.DMA((29,)),
            pltpu.SemaphoreType.DMA((2,)),
        ],
        compiler_params=pltpu.CompilerParams(
            collective_id=0, has_side_effects=True, vmem_limit_bytes=60 * 2**20
        ),
        name="front",
    )(
        queries, key_rows, value_rows, doc_ids.reshape(8, 1, 128), sink_logit,
        norm_gain.reshape(1, 2048), residual, out_weight,
    )


def per_device(
    queries,
    key_rows,
    value_rows,
    doc_ids,
    sink_logit,
    residual,
    out_weight,
    norm_gain,
    gate_weight,
    up_weight,
    down_weight,
    routes,
    route_weights,
):
    stream, normed = front(
        queries, key_rows, value_rows, doc_ids, sink_logit, residual, out_weight, norm_gain
    )
    stream_f = stream.astype(jnp.float32)
    home_rows = normed.shape[0]
    width = normed.shape[1]
    route_count = routes.shape[1]
    expert_count = lax.axis_size("sp") * gate_weight.shape[0]
    capacity = route_count * home_rows // expert_count
    flat_routes = routes.reshape(-1)
    one_hot = (flat_routes[:, None] == jnp.arange(expert_count, dtype=jnp.int32)[None, :]).astype(
        jnp.int32
    )
    earlier = jnp.cumsum(one_hot, axis=0) - one_hot
    slot_rank = jnp.sum(earlier * one_hot, axis=1)
    slot_index = flat_routes * capacity + slot_rank
    source_row = (
        jnp.zeros((expert_count * capacity,), jnp.int32)
        .at[slot_index]
        .set(jnp.arange(home_rows * route_count, dtype=jnp.int32) // route_count)
    )
    outgoing = normed[source_row].reshape(expert_count, capacity, width)
    incoming = lax.all_to_all(outgoing, "sp", split_axis=0, concat_axis=0, tiled=True)
    flat_rows = incoming.reshape(-1, width)
    gate_act = jnp.dot(flat_rows, gate_weight[0], preferred_element_type=jnp.float32)
    up_act = jnp.dot(flat_rows, up_weight[0], preferred_element_type=jnp.float32)
    hidden = (jax.nn.silu(gate_act) * up_act).astype(jnp.bfloat16)
    produced = jnp.dot(hidden, down_weight[0], preferred_element_type=jnp.float32).astype(
        jnp.bfloat16
    )
    returned = lax.all_to_all(
        produced.reshape(incoming.shape), "sp", split_axis=0, concat_axis=0, tiled=True
    )
    route_out = returned.reshape(-1, width)[slot_index].reshape(home_rows, route_count, width)
    weighted = jnp.sum(route_weights[:, :, None] * route_out.astype(jnp.float32), axis=1)
    return (stream_f + weighted).astype(jnp.bfloat16)


def solution(mesh):
    return jax.shard_map(
        per_device,
        mesh=mesh,
        in_specs=(
            P("sp", "tp"),
            P("sp", "tp"),
            P("sp", "tp"),
            P("sp"),
            P("tp"),
            P(("sp", "tp"), None),
            P("tp", None),
            P(),
            P("sp", None, None),
            P("sp", None, None),
            P("sp", None, None),
            P(("sp", "tp"), None),
            P(("sp", "tp"), None),
        ),
        out_specs=P(("sp", "tp"), None),
        check_vma=False,
    )
```

```python
import jax
import jax.numpy as jnp
from jax import lax
from jax.experimental import pallas as pl
from jax.experimental.pallas import tpu as pltpu
from jax.sharding import PartitionSpec as P

HD = 64
BLK = 128
MESH = pl.DeviceIdType.MESH
NEG = -1e30
EPS = 1e-06
BF = jnp.bfloat16
F32 = jnp.float32


def coords():
    s = lax.axis_index("sp")
    y = lax.axis_index("tp")
    c = lax.rem(s, 2)
    x = lax.rem(s // 2, 4)
    z = s // 8
    return s, y, z, x, c


def sp_of(z, x, c):
    return (z * 4 + x) * 2 + c


def front_kernel(
    q_ref, k_ref, v_ref, docs_ref, sink_ref, gain_ref, resid_hbm, w_hbm,
    stream_ref, normed_ref,
    k2, v2, dpad, khalo, vhalo, att, regr, wall, w_own, resid, acc, bias,
    send, recv, lsem,
):
    s, y, z, x, c = coords()
    xm, xp = lax.rem(x + 3, 4), lax.rem(x + 1, 4)
    xo = lax.rem(x + 2, 4)
    sp_next = (lax.rem(s + 1, 64), y)
    sp_prev = (lax.rem(s + 63, 64), y)
    sib = (sp_of(z, x, 1 - c), y)
    x_next = (sp_of(z, xp, c), y)
    x_prev = (sp_of(z, xm, c), y)
    tps = [None] + [(s, lax.rem(y + r, 4)) for r in (1, 2, 3)]

    def rc(src, dst, n, dev):
        return pltpu.make_async_remote_copy(
            src_ref=src, dst_ref=dst, send_sem=send.at[n], recv_sem=recv.at[n],
            device_id=dev, device_id_type=MESH,
        )

    started = []

    def go(src, dst, n, dev):
        d = rc(src, dst, n, dev)
        d.start()
        started.append(d)

    def got(dst, n):
        rc(dst, dst, n, sib).wait_recv()

    w_copy = pltpu.make_async_copy(w_hbm, w_own, lsem.at[0])
    r_copy = pltpu.make_async_copy(resid_hbm, resid, lsem.at[1])
    w_copy.start()
    r_copy.start()
    barrier = pltpu.get_barrier_semaphore()
    for dev in (sp_next, sp_prev, tps[1], tps[2], tps[3], x_next, x_prev):
        pl.semaphore_signal(barrier, inc=1, device_id=dev, device_id_type=MESH)
    pl.semaphore_wait(barrier, 7)

    go(k_ref.at[pl.ds(896, 128)], khalo.at[0], 0, sp_next)
    go(v_ref.at[pl.ds(896, 128)], vhalo.at[0], 1, sp_next)
    go(docs_ref.at[7], dpad.at[0], 2, sp_next)
    go(k_ref.at[pl.ds(0, 128)], khalo.at[1], 3, sp_prev)
    go(v_ref.at[pl.ds(0, 128)], vhalo.at[1], 4, sp_prev)
    go(docs_ref.at[0], dpad.at[9], 5, sp_prev)

    def rows(xx, cc, off, n):
        return pl.ds(pl.multiple_of(128 * xx + 64 * cc + off, 32), n)

    w_copy.wait()
    mine = rows(x, c, 0, 64)
    mine_lo, mine_hi = rows(x, c, 0, 32), rows(x, c, 32, 32)
    go(w_own.at[mine], wall.at[0, mine], 6, tps[1])
    go(w_own.at[mine], wall.at[1, mine], 7, tps[3])

    lane = lax.broadcasted_iota(jnp.int32, (BLK, BLK), 1)
    row = lax.broadcasted_iota(jnp.int32, (BLK, BLK), 0)
    low = lane < 64

    def dup(src, dst, at):
        v = src.astype(F32)
        rolled = pltpu.roll(v, 64, 1)
        dst[0, pl.ds(at, BLK), :] = jnp.where(low, v, rolled).astype(BF)
        dst[1, pl.ds(at, BLK), :] = jnp.where(low, rolled, v).astype(BF)

    @pl.loop(0, 8)
    def _(i):
        at = pl.multiple_of(i * BLK, BLK)
        dup(k_ref[pl.ds(at, BLK), :], k2, at + BLK)
        dup(v_ref[pl.ds(at, BLK), :], v2, at + BLK)
        dpad[i + 1] = docs_ref[i]

    for n, ref in ((0, khalo.at[0]), (1, vhalo.at[0]), (2, dpad.at[0]),
                   (3, khalo.at[1]), (4, vhalo.at[1]), (5, dpad.at[9])):
        got(ref, n)
    dup(khalo[0], k2, 0)
    dup(khalo[1], k2, 9 * BLK)
    dup(vhalo[0], v2, 0)
    dup(vhalo[1], v2, 9 * BLK)
    dpad[0] = jnp.where(s == 0, -1, dpad[0])
    dpad[9] = jnp.where(s == 63, -1, dpad[9])

    scale = HD ** (-0.5)
    mrow = lax.broadcasted_iota(jnp.int32, (BLK, BLK), 1)
    m_even = jnp.where(mrow < 64, scale, 0.0).astype(BF)
    m_odd = jnp.where(mrow < 64, 0.0, scale).astype(BF)

    def pair_of_blocks(t, out, out_at):
        p = lax.rem(y + 1 + t, 4)

        @pl.loop(0, 4)
        def _(it):
            sub = it // 2
            g = lax.rem(it, 2)
            b = 2 * p + sub
            at = pl.multiple_of(b * BLK, BLK)

            @pl.when(g == 0)
            def _():
                qd = jnp.transpose(jnp.broadcast_to(dpad[b + 1].astype(F32), (BLK, BLK)))
                for j in range(3):
                    ok = qd == dpad[b + j].astype(F32)
                    if j == 0:
                        ok = ok & (lane >= row)
                    if j == 2:
                        ok = ok & (lane <= row)
                    bias[:, j * BLK:(j + 1) * BLK] = jnp.where(ok, 0.0, NEG)

            keys = k2[g, pl.ds(at, 3 * BLK), :]
            vals = v2[g, pl.ds(at, 3 * BLK), :]
            for pair in range(2):
                col = pl.multiple_of(g * 256 + pair * BLK, BLK)
                qq = q_ref[pl.ds(at, BLK), pl.ds(col, BLK)]
                outs = []
                for half in range(2):
                    sink = sink_ref[g * 4 + pair * 2 + half]
                    qm = qq * (m_even if half == 0 else m_odd)
                    sc = lax.dot_general(qm, keys, (((1,), (1,)), ((), ())),
                                         preferred_element_type=F32) + bias[...]
                    top = jnp.maximum(jnp.max(sc, axis=1, keepdims=True), sink)
                    ex = jnp.exp(sc - top)
                    den = jnp.sum(ex, axis=1, keepdims=True) + jnp.exp(sink - top)
                    o = jnp.dot(ex.astype(BF), vals, preferred_element_type=F32)
                    outs.append(o * (1.0 / den))
                out[out_at, pl.ds(pl.multiple_of(sub * BLK, BLK), BLK), pl.ds(col, BLK)] = (
                    jnp.where(low, outs[0], outs[1]).astype(BF))

    def send_att(t):
        r = t + 1
        go(att.at[t], regr.at[4 - r], 26 + t, tps[r])

    ab, dd = pl.ds(0, 2), pl.ds(2, 1)
    pair_of_blocks(0, att, 0)
    got(wall.at[0, mine], 6)
    got(wall.at[1, mine], 7)
    go(wall.at[0, mine_lo], wall.at[2, mine_lo], 8, tps[1])
    go(wall.at[1, mine_hi], wall.at[2, mine_hi], 9, tps[3])
    go(wall.at[ab, mine], wall.at[ab, mine], 10, x_next)
    go(wall.at[ab, mine], wall.at[ab, mine], 11, x_prev)
    go(wall.at[ab, mine], wall.at[ab, mine], 18, sib)
    pair_of_blocks(1, att, 1)
    send_att(0)
    pair_of_blocks(2, att, 2)
    send_att(1)
    got(wall.at[2, mine_lo], 8)
    got(wall.at[2, mine_hi], 9)
    go(wall.at[dd, mine], wall.at[dd, mine], 12, x_next)
    go(wall.at[dd, mine], wall.at[dd, mine], 13, x_prev)
    go(wall.at[dd, mine], wall.at[dd, mine], 19, sib)
    pair_of_blocks(3, regr, 0)
    send_att(2)

    from_m, from_p = rows(xm, c, 0, 64), rows(xp, c, 0, 64)
    fm_lo, fp_hi = rows(xm, c, 0, 32), rows(xp, c, 32, 32)
    far, far_lo, far_hi = rows(xo, c, 0, 64), rows(xo, c, 0, 32), rows(xo, c, 32, 32)

    for sh, n, nd in ((ab, 10, 20), (dd, 12, 21)):
        got(wall.at[sh, from_m], n)
        got(wall.at[sh, from_p], n + 1)
        go(wall.at[sh, fm_lo], wall.at[sh, fm_lo], n + 4, x_next)
        go(wall.at[sh, fp_hi], wall.at[sh, fp_hi], n + 5, x_prev)
        go(wall.at[sh, from_m], wall.at[sh, from_m], nd, sib)
        go(wall.at[sh, from_p], wall.at[sh, from_p], nd + 2, sib)

    r_copy.wait()
    acc[...] = resid[...].astype(F32)

    def project(r, wref):
        @pl.loop(0, 4)
        def _(n):
            cols = pl.ds(pl.multiple_of(n * 512, 512), 512)
            part = jnp.dot(regr[r], wref[:, cols], preferred_element_type=F32)
            acc[:, cols] += part.astype(BF).astype(F32)

    project(0, w_own)
    for sh, n, nd in ((ab, 14, 24), (dd, 16, 25)):
        got(wall.at[sh, far_lo], n)
        got(wall.at[sh, far_hi], n + 1)
        go(wall.at[sh, far], wall.at[sh, far], nd, sib)
        for xx, m in ((x, nd - 6), (xm, nd - 4), (xp, nd - 2), (xo, nd)):
            sl = rows(xx, 1 - c, 0, 64)
            got(wall.at[sh, sl], m)
        if n == 14:
            got(regr.at[1], 26 + 2)
            project(1, wall.at[1])
            got(regr.at[3], 26)
            project(3, wall.at[0])
        else:
            got(regr.at[2], 26 + 1)
            project(2, wall.at[2])

    @pl.loop(0, 16)
    def _(i):
        rr = pl.ds(pl.multiple_of(i * 16, 16), 16)
        st = acc[rr, :].astype(BF)
        stream_ref[rr, :] = st
        sf = st.astype(F32)
        sc = lax.rsqrt(jnp.mean(sf * sf, axis=1, keepdims=True) + EPS)
        normed_ref[rr, :] = (sf * sc * gain_ref[...]).astype(BF)

    for d in started:
        d.wait_send()


def front(queries, key_rows, value_rows, doc_ids, sink_logit, residual, out_weight, norm_gain):
    vm = pl.BlockSpec(memory_space=pltpu.VMEM)
    anyspec = pl.BlockSpec(memory_space=pl.ANY)
    return pl.pallas_call(
        front_kernel,
        out_shape=(
            jax.ShapeDtypeStruct((256, 2048), BF),
            jax.ShapeDtypeStruct((256, 2048), BF),
        ),
        in_specs=[vm, vm, vm, vm, pl.BlockSpec(memory_space=pltpu.SMEM), vm, anyspec, anyspec],
        out_specs=(vm, vm),
        scratch_shapes=[
            pltpu.VMEM((2, 1280, 128), BF),
            pltpu.VMEM((2, 1280, 128), BF),
            pltpu.VMEM((10, 1, 128), jnp.int32),
            pltpu.VMEM((2, 128, 128), BF),
            pltpu.VMEM((2, 128, 128), BF),
            pltpu.VMEM((3, 256, 512), BF),
            pltpu.VMEM((4, 256, 512), BF),
            pltpu.VMEM((3, 512, 2048), BF),
            pltpu.VMEM((512, 2048), BF),
            pltpu.VMEM((256, 2048), BF),
            pltpu.VMEM((256, 2048), F32),
            pltpu.VMEM((128, 384), F32),
            pltpu.SemaphoreType.DMA((29,)),
            pltpu.SemaphoreType.DMA((29,)),
            pltpu.SemaphoreType.DMA((2,)),
        ],
        compiler_params=pltpu.CompilerParams(
            collective_id=0, has_side_effects=True, vmem_limit_bytes=60 * 2**20
        ),
        name="front",
    )(
        queries, key_rows, value_rows, doc_ids.reshape(8, 1, 128), sink_logit,
        norm_gain.reshape(1, 2048), residual, out_weight,
    )


PAIRS = ((0, 4), (1, 2), (3, 5), (6, 7))


def moe_kernel(
    normed_ref, stream_ref, routes_ref, rw_ref, gate_hbm, up_hbm, down_hbm,
    mixed_ref,
    sbuf, land, metas, metar, mscr, pg_t, whi, wlo, xbuf, xin, pbuf, rbuf,
    partk, psend, cback, totb, fin, wg, wu, wd, send, recv, lsem,
):
    s, y, z, x, c = coords()
    me = 2 * x + c
    zl = lax.rem(z, 2)
    g_me = z // 2
    sgn = 2 * zl - 1

    def zdev(zz):
        return (sp_of(lax.rem(zz + 16, 8), x, c), y)

    def xdev(i):
        i = lax.rem(i + 8, 8)
        return (sp_of(z, i // 2, lax.rem(i, 2)), y)

    partner = zdev(z - sgn)

    def rc(src, dst, n, dev):
        return pltpu.make_async_remote_copy(
            src_ref=src, dst_ref=dst, send_sem=send.at[n], recv_sem=recv.at[n],
            device_id=dev, device_id_type=MESH,
        )

    pending = []

    def go(src, dst, n, dev, note=True):
        d = rc(src, dst, n, dev)
        d.start()
        if note:
            pending.append(d)

    def got(dst, n):
        rc(dst, dst, n, partner).wait_recv()

    loads = [pltpu.make_async_copy(a, b, lsem.at[i])
             for i, (a, b) in enumerate(((gate_hbm.at[0], wg), (up_hbm.at[0], wu), (down_hbm.at[0], wd)))]
    for cp in loads:
        cp.start()
    barrier = pltpu.get_barrier_semaphore()
    for o in range(1, 8):
        pl.semaphore_signal(barrier, inc=1, device_id=zdev(z + o), device_id_type=MESH)
        pl.semaphore_signal(barrier, inc=1, device_id=xdev(me + o), device_id_type=MESH)

    e0, e1 = routes_ref[0:1, :], routes_ref[1:2, :]
    upper = (lax.broadcasted_iota(jnp.int32, (256, 256), 0)
             < lax.broadcasted_iota(jnp.int32, (256, 256), 1)).astype(F32).astype(BF)
    ei = lax.broadcasted_iota(jnp.int32, (64, 256), 0)
    h0 = (ei == e0).astype(F32)
    h1 = (ei == e1).astype(F32)
    hg = (lax.broadcasted_iota(jnp.int32, (16, 256), 0) == (e0 >> 4)).astype(F32)

    def before(h):
        return jnp.dot(h.astype(BF), upper, preferred_element_type=F32)

    rank0 = jnp.sum(h0 * before(h0), axis=0, keepdims=True)
    rank1 = jnp.sum(h1 * (before(h1) + jnp.sum(h0, axis=1, keepdims=True)), axis=0, keepdims=True)
    gpos = jnp.sum(hg * before(hg), axis=0, keepdims=True) + ((e0 >> 4) * 64).astype(F32)
    w0, w1 = rw_ref[0:1, :], rw_ref[1:2, :]
    w0h = w0.astype(BF).astype(F32)
    w1h = w1.astype(BF).astype(F32)
    mscr[...] = jnp.zeros((16, 256), F32)
    mscr[0:1, :] = ((e0 & 15) * 8).astype(F32) + rank0
    mscr[1:2, :] = ((e1 & 15) * 8).astype(F32) + rank1
    mscr[2:3, :] = w0h
    mscr[3:4, :] = w0 - w0h
    mscr[4:5, :] = w1h
    mscr[5:6, :] = w1 - w1h
    pg = (lax.broadcasted_iota(jnp.int32, (256, 256), 0).astype(F32) == gpos).astype(F32)
    pg_t[...] = jnp.transpose(pg).astype(BF)
    pgb = pg.astype(BF)
    info = mscr[...].astype(BF)
    for g in range(4):
        pgg = pgb[64 * g:64 * (g + 1), :]
        both = jnp.concatenate([pgg, pgg], axis=0)
        metas[g] = lax.dot_general(info, both, (((1,), (1,)), ((), ())),
                                   preferred_element_type=F32)[0:8, :]

    @pl.loop(0, 8)
    def _(n):
        cols = pl.ds(pl.multiple_of(n * 256, 256), 256)
        out = jnp.dot(pgb, normed_ref[:, cols], preferred_element_type=F32).astype(BF)
        for g in range(4):
            sbuf[g, :, cols] = out[64 * g:64 * (g + 1), :]

    pl.semaphore_wait(barrier, 14)

    g_of = [g_me, lax.rem(g_me + sgn + 4, 4), lax.rem(g_me - sgn + 4, 4), lax.rem(g_me + 2, 4)]
    t_of = [None, z + sgn, z - 2 * sgn, z + 3 * sgn]
    for o in range(1, 8):
        zz = lax.rem(z + o, 8)
        go(metas.at[zz // 2], metar.at[o], o, zdev(z + o))
    metar[0] = metas[g_me]
    go(sbuf.at[g_of[1]], land.at[1], 9, zdev(t_of[1]))
    go(sbuf.at[g_me], land.at[4], 8, partner)
    go(sbuf.at[g_of[3]], land.at[3], 11, zdev(t_of[3]))
    go(sbuf.at[g_of[2]], land.at[2], 10, zdev(t_of[2]))
    for o in range(1, 8):
        got(metar.at[o], o)

    def origin(b):
        if b == 0:
            return 0
        if b < 4:
            return lax.rem(8 - sgn * b, 8)
        return lax.rem(8 + sgn * (b - 3), 8)

    def fwd(k):
        got(land.at[k], 8 + k)
        go(land.at[k], land.at[4 + k], 11 + k, partner)

    lane = lax.broadcasted_iota(jnp.int32, (128, 128), 1)
    ii = lax.broadcasted_iota(jnp.int32, (128, 128), 0)

    def exchange(p):
        b0, b1 = PAIRS[p]
        mm = jnp.where(lane[0:8, :] < 64, metar[origin(b0)], metar[origin(b1)])
        slot = ((((ii >> 4) + me) & 7) << 3) + (ii & 7) + 64 * zl
        slot = jnp.where(((ii >> 3) & 1) == (lane >> 6), slot, -1).astype(F32)
        hit0 = slot == mm[0:1, :]
        hit1 = slot == mm[1:2, :]
        sel = jnp.where(hit0 | hit1, 1.0, 0.0).astype(BF)
        for r, ref in ((2, whi), (3, wlo)):
            wt = jnp.where(hit0, mm[r:r + 1, :], 0.0) + jnp.where(hit1, mm[r + 2:r + 3, :], 0.0)
            ref[p] = jnp.transpose(wt).astype(BF)
        first = sbuf.at[g_me] if b0 == 0 else land.at[b0]

        @pl.loop(0, 4)
        def _(n):
            cols = pl.ds(pl.multiple_of(n * 512, 512), 512)
            rows = jnp.concatenate([first[:, cols], land[b1, :, cols]], axis=0)
            out = jnp.dot(sel, rows, preferred_element_type=F32).astype(BF)
            xbuf[p, :, cols] = out
            xin[p, 0:16, cols] = out[0:16, :]

        for o in (2, 6, 4, 5, 3, 7, 1):
            sl = pl.ds(16 * o, 16)
            go(xbuf.at[p, sl], xin.at[p, sl], 15 + p, xdev(me + o), note=False)

    rest = pl.ds(16, 112)

    def expert(p):
        got(xin.at[p, rest], 15 + p)
        rows = xin[p]
        gate_act = jnp.dot(rows, wg[...], preferred_element_type=F32)
        up_act = jnp.dot(rows, wu[...], preferred_element_type=F32)
        hidden = (gate_act / (1.0 + jnp.exp(-gate_act)) * up_act).astype(BF)

        @pl.loop(0, 4)
        def _(n):
            cols = pl.ds(pl.multiple_of(n * 512, 512), 512)
            out = jnp.dot(hidden, wd[:, cols], preferred_element_type=F32).astype(BF)
            pbuf[p, :, cols] = out
            rbuf[p, 0:16, cols] = out[0:16, :]

        for o in (2, 6, 4, 5, 3, 7, 1):
            sl = pl.ds(16 * o, 16)
            go(pbuf.at[p, sl], rbuf.at[p, sl], 19 + p, xdev(me - o), note=False)

    def merge(p):
        got(rbuf.at[p, rest], 19 + p)

        @pl.loop(0, 4)
        def _(n):
            cols = pl.ds(pl.multiple_of(n * 512, 512), 512)
            rows = rbuf[p, :, cols]
            out = (jnp.dot(whi[p], rows, preferred_element_type=F32)
                   + jnp.dot(wlo[p], rows, preferred_element_type=F32))
            for h, b in enumerate(PAIRS[p]):
                piece = out[64 * h:64 * (h + 1), :]
                if b < 4:
                    partk[b, :, cols] = piece
                else:
                    psend[b - 4, :, cols] = piece.astype(BF)

        for b in PAIRS[p]:
            if b >= 4:
                go(psend.at[b - 4], cback.at[b - 4], 19 + b, partner)

    def total(j):
        got(cback.at[j], 23 + j)

        @pl.loop(0, 4)
        def _(n):
            cols = pl.ds(pl.multiple_of(n * 512, 512), 512)
            out = (partk[j, :, cols] + cback[j, :, cols].astype(F32)).astype(BF)
            if j == 0:
                fin[g_me, :, cols] = out
            else:
                totb[j - 1, :, cols] = out

        if j:
            go(totb.at[j - 1], fin.at[g_me], 26 + j, zdev(z + sgn * j))

    fwd(1)
    got(land.at[4], 8)
    exchange(0)
    fwd(2)
    exchange(1)
    for cp in loads:
        cp.wait()
    expert(0)
    fwd(3)
    got(land.at[5], 12)
    exchange(2)
    expert(1)
    merge(0)
    expert(2)
    merge(1)
    got(land.at[6], 13)
    got(land.at[7], 14)
    exchange(3)
    merge(2)
    total(0)
    expert(3)
    total(1)
    merge(3)
    total(2)
    total(3)
    for k in (1, 2, 3):
        got(fin.at[g_of[k]], 26 + k)

    @pl.loop(0, 8)
    def _(n):
        cols = pl.ds(pl.multiple_of(n * 256, 256), 256)
        out = stream_ref[:, cols].astype(F32)
        rows = jnp.concatenate([fin[g, :, cols] for g in range(4)], axis=0)
        out += jnp.dot(pg_t[...], rows, preferred_element_type=F32)
        mixed_ref[:, cols] = out.astype(BF)

    for d in pending:
        d.wait_send()
    for p in range(4):
        rc(xbuf.at[p, rest], xbuf.at[p, rest], 15 + p, partner).wait_send()
        rc(pbuf.at[p, rest], pbuf.at[p, rest], 19 + p, partner).wait_send()


def moe(normed, stream, routes, route_weights, gate_weight, up_weight, down_weight):
    vm = pl.BlockSpec(memory_space=pltpu.VMEM)
    anyspec = pl.BlockSpec(memory_space=pl.ANY)
    big = (4, 128, 2048)
    return pl.pallas_call(
        moe_kernel,
        out_shape=jax.ShapeDtypeStruct((256, 2048), BF),
        in_specs=[vm, vm, vm, vm, anyspec, anyspec, anyspec],
        out_specs=vm,
        scratch_shapes=[
            pltpu.VMEM((4, 64, 2048), BF),
            pltpu.VMEM((8, 64, 2048), BF),
            pltpu.VMEM((4, 8, 128), F32),
            pltpu.VMEM((8, 8, 128), F32),
            pltpu.VMEM((16, 256), F32),
            pltpu.VMEM((256, 256), BF),
            pltpu.VMEM((4, 128, 128), BF),
            pltpu.VMEM((4, 128, 128), BF),
            pltpu.VMEM(big, BF),
            pltpu.VMEM(big, BF),
            pltpu.VMEM(big, BF),
            pltpu.VMEM(big, BF),
            pltpu.VMEM((4, 64, 2048), F32),
            pltpu.VMEM((4, 64, 2048), BF),
            pltpu.VMEM((4, 64, 2048), BF),
            pltpu.VMEM((3, 64, 2048), BF),
            pltpu.VMEM((4, 64, 2048), BF),
            pltpu.VMEM((2048, 512), BF),
            pltpu.VMEM((2048, 512), BF),
            pltpu.VMEM((512, 2048), BF),
            pltpu.SemaphoreType.DMA((30,)),
            pltpu.SemaphoreType.DMA((30,)),
            pltpu.SemaphoreType.DMA((3,)),
        ],
        compiler_params=pltpu.CompilerParams(
            collective_id=1, has_side_effects=True, vmem_limit_bytes=60 * 2**20
        ),
        name="moe",
    )(normed, stream, routes.T, route_weights.T, gate_weight, up_weight, down_weight)


def per_device(
    queries,
    key_rows,
    value_rows,
    doc_ids,
    sink_logit,
    residual,
    out_weight,
    norm_gain,
    gate_weight,
    up_weight,
    down_weight,
    routes,
    route_weights,
):
    stream, normed = front(
        queries, key_rows, value_rows, doc_ids, sink_logit, residual, out_weight, norm_gain
    )
    return moe(normed, stream, routes, route_weights, gate_weight, up_weight, down_weight)


def solution(mesh):
    return jax.shard_map(
        per_device,
        mesh=mesh,
        in_specs=(
            P("sp", "tp"),
            P("sp", "tp"),
            P("sp", "tp"),
            P("sp"),
            P("tp"),
            P(("sp", "tp"), None),
            P("tp", None),
            P(),
            P("sp", None, None),
            P("sp", None, None),
            P("sp", None, None),
            P(("sp", "tp"), None),
            P(("sp", "tp"), None),
        ),
        out_specs=P(("sp", "tp"), None),
        check_vma=False,
    )
```

```python
import jax
import jax.numpy as jnp
from jax import lax
from jax.experimental import pallas as pl
from jax.experimental.pallas import tpu as pltpu
from jax.sharding import PartitionSpec as P

HD = 64
BLK = 128
MESH = pl.DeviceIdType.MESH
NEG = -1e30
EPS = 1e-06
BF = jnp.bfloat16
F32 = jnp.float32


def coords():
    s = lax.axis_index("sp")
    y = lax.axis_index("tp")
    c = lax.rem(s, 2)
    x = lax.rem(s // 2, 4)
    z = s // 8
    return s, y, z, x, c


def sp_of(z, x, c):
    return (z * 4 + x) * 2 + c


PAIRS = ((0, 1), (2, 3), (5, 6), (7, 4))


def layer_kernel(
    q_ref, k_ref, v_ref, docs_ref, sink_ref, gain_ref, routes_ref, rw_ref,
    resid_hbm, w_hbm, gate_hbm, up_hbm, down_hbm,
    mixed_ref,
    k2, v3, dpad, khalo, vhalo, att, regr, wall, w_own, resid, acc, bias, scores, probs, squares,
    stream, sbuf, land, metas, metar, mscr, pg_n, pg_t, whi, wlo, xbuf, xin, pbuf, rbuf,
    partk, psend, cback, totb, fin, wg, wu, wd, fsend, frecv, msend, mrecv, lsem,
):
    s, y, z, x, c = coords()
    xm, xp = lax.rem(x + 3, 4), lax.rem(x + 1, 4)
    xo = lax.rem(x + 2, 4)
    me = 2 * x + c
    zl = lax.rem(z, 2)
    g_me = z // 2
    sgn = 2 * zl - 1

    def zdev(zz):
        return (sp_of(lax.rem(zz + 16, 8), x, c), y)

    def xdev(i):
        i = lax.rem(i + 8, 8)
        return (sp_of(z, i // 2, lax.rem(i, 2)), y)

    sp_next = (lax.rem(s + 1, 64), y)
    sp_prev = (lax.rem(s + 63, 64), y)
    sib = (sp_of(z, x, 1 - c), y)
    x_next = (sp_of(z, xp, c), y)
    x_prev = (sp_of(z, xm, c), y)
    z_next, z_prev = zdev(z + 1), zdev(z - 1)
    tps = [None] + [(s, lax.rem(y + r, 4)) for r in (1, 2, 3)]
    partner = zdev(z - sgn)

    def rc(src, dst, n, dev):
        return pltpu.make_async_remote_copy(
            src_ref=src, dst_ref=dst, send_sem=fsend.at[n], recv_sem=frecv.at[n],
            device_id=dev, device_id_type=MESH,
        )

    pending = []

    def go(src, dst, n, dev):
        d = rc(src, dst, n, dev)
        d.start()
        pending.append(d)

    def got(dst, n):
        rc(dst, dst, n, sib).wait_recv()


    def mrc(src, dst, n, dev):
        return pltpu.make_async_remote_copy(
            src_ref=src, dst_ref=dst, send_sem=msend.at[n], recv_sem=mrecv.at[n],
            device_id=dev, device_id_type=MESH,
        )

    def mgo(src, dst, n, dev, note=True):
        d = mrc(src, dst, n, dev)
        d.start()
        if note:
            pending.append(d)

    def mgot(dst, n):
        mrc(dst, dst, n, partner).wait_recv()

    w_copy = pltpu.make_async_copy(w_hbm, w_own, lsem.at[0])
    r_copy = pltpu.make_async_copy(resid_hbm, resid, lsem.at[1])
    w_copy.start()
    r_copy.start()
    loads = [pltpu.make_async_copy(a, b, lsem.at[2 + i])
             for i, (a, b) in enumerate(((gate_hbm.at[0], wg), (up_hbm.at[0], wu), (down_hbm.at[0], wd)))]
    for cp in loads:
        cp.start()
    barrier = pltpu.get_barrier_semaphore()
    greet = [sp_next, sp_prev, tps[1], tps[2], tps[3]]
    greet += [zdev(z + o) for o in range(1, 8)] + [xdev(me + o) for o in range(1, 8)]
    for dev in greet:
        pl.semaphore_signal(barrier, inc=1, device_id=dev, device_id_type=MESH)
    pl.semaphore_wait(barrier, len(greet))

    go(k_ref.at[pl.ds(896, 128)], khalo.at[0], 0, sp_next)
    go(v_ref.at[pl.ds(896, 128)], vhalo.at[0], 1, sp_next)
    go(docs_ref.at[7], dpad.at[0], 2, sp_next)
    go(k_ref.at[pl.ds(0, 128)], khalo.at[1], 3, sp_prev)
    go(v_ref.at[pl.ds(0, 128)], vhalo.at[1], 4, sp_prev)
    go(docs_ref.at[0], dpad.at[9], 5, sp_prev)

    def rows_a(xx, cc, off, n):
        return pl.ds(pl.multiple_of(64 * xx + 32 * cc + off, 16), n)

    def rows_b(zz, cc):
        return pl.ds(pl.multiple_of(256 + 32 * lax.rem(zz + 16, 8) + 16 * cc, 16), 16)

    left, right = pl.ds(0, 1024), pl.ds(1024, 1024)
    w_copy.wait()
    mine = rows_a(x, c, 0, 32)
    mine_lo, mine_hi = rows_a(x, c, 0, 16), rows_a(x, c, 16, 16)
    mine_b = rows_b(z, c)
    go(w_own.at[mine], wall.at[0, mine], 6, tps[1])
    go(w_own.at[mine], wall.at[1, mine], 7, tps[3])
    go(w_own.at[mine_b], wall.at[0, mine_b], 30, tps[1])
    go(w_own.at[mine_b], wall.at[1, mine_b], 31, tps[3])

    e0, e1 = routes_ref[0:1, :], routes_ref[1:2, :]
    upper = (lax.broadcasted_iota(jnp.int32, (256, 256), 0)
             < lax.broadcasted_iota(jnp.int32, (256, 256), 1)).astype(F32).astype(BF)
    ei = lax.broadcasted_iota(jnp.int32, (64, 256), 0)
    h0 = (ei == e0).astype(F32)
    h1 = (ei == e1).astype(F32)
    hg = (lax.broadcasted_iota(jnp.int32, (16, 256), 0) == (e0 >> 4)).astype(F32)

    def before(h):
        return jnp.dot(h.astype(BF), upper, preferred_element_type=F32)

    rank0 = jnp.sum(h0 * before(h0), axis=0, keepdims=True)
    rank1 = jnp.sum(h1 * (before(h1) + jnp.sum(h0, axis=1, keepdims=True)), axis=0, keepdims=True)
    gpos = jnp.sum(hg * before(hg), axis=0, keepdims=True) + ((e0 >> 4) * 64).astype(F32)
    w0, w1 = rw_ref[0:1, :], rw_ref[1:2, :]
    w0h = w0.astype(BF).astype(F32)
    w1h = w1.astype(BF).astype(F32)
    mscr[...] = jnp.zeros((16, 256), F32)
    mscr[0:1, :] = ((e0 & 15) * 8).astype(F32) + rank0
    mscr[1:2, :] = ((e1 & 15) * 8).astype(F32) + rank1
    mscr[2:3, :] = w0h
    mscr[3:4, :] = w0 - w0h
    mscr[4:5, :] = w1h
    mscr[5:6, :] = w1 - w1h
    pg = (lax.broadcasted_iota(jnp.int32, (256, 256), 0).astype(F32) == gpos).astype(F32)
    pg_t[...] = jnp.transpose(pg).astype(BF)
    pgb = pg.astype(BF)
    pg_n[...] = pgb
    info = mscr[...].astype(BF)
    for g in range(4):
        pgg = pgb[64 * g:64 * (g + 1), :]
        both = jnp.concatenate([pgg, pgg], axis=0)
        metas[g] = lax.dot_general(info, both, (((1,), (1,)), ((), ())),
                                   preferred_element_type=F32)[0:8, :]

    for o in range(1, 8):
        zz = lax.rem(z + o, 8)
        mgo(metas.at[zz // 2], metar.at[o], o, zdev(z + o))
    metar[0] = metas[g_me]

    lane = lax.broadcasted_iota(jnp.int32, (BLK, BLK), 1)
    row = lax.broadcasted_iota(jnp.int32, (BLK, BLK), 0)
    low = lane < 64

    def dup(src, dst, at):
        v = src.astype(F32)
        rolled = pltpu.roll(v, 64, 1)
        dst[0, pl.ds(at, BLK), 0:BLK] = jnp.where(low, v, rolled).astype(BF)
        dst[1, pl.ds(at, BLK), 0:BLK] = jnp.where(low, rolled, v).astype(BF)

    @pl.loop(0, 8)
    def _(i):
        at = pl.multiple_of(i * BLK, BLK)
        dup(k_ref[pl.ds(at, BLK), :], k2, at + BLK)
        dup(v_ref[pl.ds(at, BLK), :], v3, at + BLK)
        dpad[i + 1] = docs_ref[i]

    @pl.loop(0, 10)
    def _(i):
        at = pl.multiple_of(i * BLK, BLK)
        for g in range(2):
            v3[g, pl.ds(at, BLK), BLK:2 * BLK] = jnp.ones((BLK, BLK), BF)

    for n, ref in ((0, khalo.at[0]), (1, vhalo.at[0]), (2, dpad.at[0]),
                   (3, khalo.at[1]), (4, vhalo.at[1]), (5, dpad.at[9])):
        got(ref, n)
    dup(khalo[0], k2, 0)
    dup(khalo[1], k2, 9 * BLK)
    dup(vhalo[0], v3, 0)
    dup(vhalo[1], v3, 9 * BLK)
    dpad[0] = jnp.where(s == 0, -1, dpad[0])
    dpad[9] = jnp.where(s == 63, -1, dpad[9])

    scale = HD ** (-0.5)
    m_even = jnp.where(low, scale, 0.0).astype(BF)
    m_odd = jnp.where(low, 0.0, scale).astype(BF)

    def pair_of_blocks(t, out, out_at):
        p = lax.rem(y + 1 + t, 4)

        @pl.loop(0, 2)
        def _(sub):
            b = 2 * p + sub
            at = pl.multiple_of(b * BLK, BLK)
            qd = jnp.transpose(jnp.broadcast_to(dpad[b + 1].astype(F32), (BLK, BLK)))
            for j in range(3):
                ok = qd == dpad[b + j].astype(F32)
                if j == 0:
                    ok = ok & (lane >= row)
                if j == 2:
                    ok = ok & (lane <= row)
                bias[:, j * BLK:(j + 1) * BLK] = jnp.where(ok, 0.0, NEG)
            for g in range(2):
                keys = k2[g, pl.ds(at, 3 * BLK), :]
                qs = []
                for pair in range(2):
                    lo_col = g * 256 + pair * BLK
                    qq = q_ref[pl.ds(at, BLK), lo_col:lo_col + BLK]
                    qs += [qq * m_even, qq * m_odd]
                sc = lax.dot_general(jnp.concatenate(qs, axis=0), keys, (((1,), (1,)), ((), ())),
                                     preferred_element_type=F32)
                for h in range(4):
                    scores[g, h * BLK:(h + 1) * BLK, :] = sc[h * BLK:(h + 1) * BLK, :] + bias[...]
            extra = {}
            for g in range(2):
                for h in range(4):
                    sink = sink_ref[g * 4 + h]
                    sc = scores[g, h * BLK:(h + 1) * BLK, :]
                    top = jnp.maximum(jnp.max(sc, axis=1, keepdims=True), sink)
                    probs[g, h * BLK:(h + 1) * BLK, :] = jnp.exp(sc - top).astype(BF)
                    extra[g, h] = jnp.exp(sink - top)
            for g in range(2):
                o = jnp.dot(probs[g], v3[g, pl.ds(at, 3 * BLK), :], preferred_element_type=F32)
                for pair in range(2):
                    res = []
                    for half in range(2):
                        h = 2 * pair + half
                        oh = o[h * BLK:(h + 1) * BLK, :]
                        res.append(oh[:, 0:BLK] / (oh[:, BLK:2 * BLK] + extra[g, h]))
                    lo_col = g * 256 + pair * BLK
                    out[out_at, pl.ds(pl.multiple_of(sub * BLK, BLK), BLK), lo_col:lo_col + BLK] = (
                        jnp.where(low, res[0], res[1]).astype(BF))

    def send_att(t):
        r = t + 1
        go(att.at[t], regr.at[4 - r], 26 + t, tps[r])

    ab, dd = pl.ds(0, 2), pl.ds(2, 1)
    parts = (ab, dd)

    def zsend(step, sh):
        for d in range(2):
            zz = z - (step - 1) if d == 0 else z + (step - 1)
            rr = rows_b(zz, c)
            ref = wall.at[parts[sh], rr] if step < 4 else wall.at[parts[sh], rr, (left, right)[d]]
            go(ref, ref, 34 + (d * 2 + sh) * 4 + step - 1, (z_next, z_prev)[d])

    def zgot(step, sh):
        for d in range(2):
            zz = z - step if d == 0 else z + step
            rr = rows_b(zz, c)
            ref = wall.at[parts[sh], rr] if step < 4 else wall.at[parts[sh], rr, (left, right)[d]]
            got(ref, 34 + (d * 2 + sh) * 4 + step - 1)

    allw = pl.ds(0, 3)
    zorder = (0, -1, 1, -2, 2, -3, 3, 4)

    def zsib(dz):
        rr = rows_b(z + dz, c)
        go(wall.at[allw, rr], wall.at[allw, rr], 50 + zorder.index(dz), sib)

    def xsib(n, xx):
        rr = rows_a(xx, c, 0, 32)
        go(wall.at[allw, rr], wall.at[allw, rr], 18 + n, sib)

    from_m, from_p = rows_a(xm, c, 0, 32), rows_a(xp, c, 0, 32)
    fm_lo, fp_hi = rows_a(xm, c, 0, 16), rows_a(xp, c, 16, 16)
    far, far_lo, far_hi = rows_a(xo, c, 0, 32), rows_a(xo, c, 0, 16), rows_a(xo, c, 16, 16)

    def xsend(sh):
        ref = wall.at[parts[sh], mine]
        go(ref, ref, 10 + 2 * sh, x_next)
        go(ref, ref, 11 + 2 * sh, x_prev)

    def xforward(sh):
        got(wall.at[parts[sh], from_m], 10 + 2 * sh)
        got(wall.at[parts[sh], from_p], 11 + 2 * sh)
        ref = wall.at[parts[sh], fm_lo]
        go(ref, ref, 14 + 2 * sh, x_next)
        ref = wall.at[parts[sh], fp_hi]
        go(ref, ref, 15 + 2 * sh, x_prev)

    pair_of_blocks(0, att, 0)
    got(wall.at[0, mine], 6)
    go(wall.at[0, mine_lo], wall.at[2, mine_lo], 8, tps[1])
    got(wall.at[1, mine], 7)
    go(wall.at[1, mine_hi], wall.at[2, mine_hi], 9, tps[3])
    got(wall.at[0, mine_b], 30)
    go(wall.at[0, mine_b, left], wall.at[2, mine_b, left], 32, tps[1])
    got(wall.at[1, mine_b], 31)
    go(wall.at[1, mine_b, right], wall.at[2, mine_b, right], 33, tps[3])
    xsend(0)
    zsend(1, 0)
    pair_of_blocks(1, att, 1)
    send_att(0)
    got(wall.at[2, mine_lo], 8)
    got(wall.at[2, mine_hi], 9)
    got(wall.at[2, mine_b, left], 32)
    got(wall.at[2, mine_b, right], 33)
    xsend(1)
    zsend(1, 1)
    xsib(0, x)
    zsib(0)
    zgot(1, 0)
    zsend(2, 0)
    pair_of_blocks(2, att, 2)
    send_att(1)
    xforward(0)
    zgot(1, 1)
    zsend(2, 1)
    zgot(2, 0)
    zsend(3, 0)
    pair_of_blocks(3, regr, 0)
    send_att(2)
    xforward(1)
    zgot(2, 1)
    zsend(3, 1)
    zgot(3, 0)
    zsend(4, 0)
    xsib(1, xm)
    xsib(2, xp)
    for dz in (-1, 1, -2, 2):
        zsib(dz)

    r_copy.wait()

    def project(r, wref, first=False):
        @pl.loop(0, 4)
        def _(n):
            cols = pl.ds(pl.multiple_of(n * 512, 512), 512)
            part = jnp.dot(regr[r], wref[:, cols], preferred_element_type=F32)
            base = resid[:, cols].astype(F32) if first else acc[:, cols]
            acc[:, cols] = base + part.astype(BF).astype(F32)

    project(0, w_own, True)
    zgot(3, 1)
    zsend(4, 1)
    zsib(-3)
    zsib(3)
    for sh in range(2):
        got(wall.at[parts[sh], far_lo], 14 + 2 * sh)
        got(wall.at[parts[sh], far_hi], 15 + 2 * sh)
    xsib(3, xo)
    zgot(4, 0)
    zgot(4, 1)
    zsib(4)
    for n, xx in enumerate((x, xm, xp, xo)):
        got(wall.at[allw, rows_a(xx, 1 - c, 0, 32)], 18 + n)
    for n, dz in enumerate(zorder):
        got(wall.at[allw, rows_b(z + dz, 1 - c)], 50 + n)
    got(regr.at[1], 28)
    got(regr.at[3], 26)
    got(regr.at[2], 27)
    project(1, wall.at[1])
    project(3, wall.at[0])
    squares[...] = jnp.zeros((256, BLK), F32)

    @pl.loop(0, 4)
    def _(n):
        cols = pl.ds(pl.multiple_of(n * 512, 512), 512)
        part = jnp.dot(regr[2], wall[2, :, cols], preferred_element_type=F32)
        st = (acc[:, cols] + part.astype(BF).astype(F32)).astype(BF)
        stream[:, cols] = st
        sq = st.astype(F32) * st.astype(F32)
        squares[...] += (sq[:, 0:128] + sq[:, 128:256]) + (sq[:, 256:384] + sq[:, 384:512])

    rms = lax.rsqrt(jnp.sum(squares[...], axis=1, keepdims=True) * (1.0 / 2048) + EPS)

    @pl.loop(0, 8)
    def _(n):
        cols = pl.ds(pl.multiple_of(n * 256, 256), 256)
        normed = (stream[:, cols].astype(F32) * rms * gain_ref[:, cols]).astype(BF)
        out = jnp.dot(pg_n[...], normed, preferred_element_type=F32).astype(BF)
        for g in range(4):
            sbuf[g, :, cols] = out[64 * g:64 * (g + 1), :]

    g_of = [g_me, lax.rem(g_me + sgn + 4, 4), lax.rem(g_me - sgn + 4, 4), lax.rem(g_me + 2, 4)]
    t_of = [None, z + sgn, z - 2 * sgn, z + 3 * sgn]
    mgo(sbuf.at[g_of[1]], land.at[1], 9, zdev(t_of[1]))
    mgo(sbuf.at[g_of[2]], land.at[2], 10, zdev(t_of[2]))
    mgo(sbuf.at[g_of[3]], land.at[3], 11, zdev(t_of[3]))
    for o in range(1, 8):
        mgot(metar.at[o], o)

    def origin(b):
        if b == 0:
            return 0
        if b < 4:
            return lax.rem(8 - sgn * b, 8)
        return lax.rem(8 + sgn * (b - 3), 8)

    def fwd(k):
        mgot(land.at[k], 8 + k)
        mgo(land.at[k], land.at[4 + k], 11 + k, partner)

    ii = lax.broadcasted_iota(jnp.int32, (128, 128), 0)

    def exchange(p):
        b0, b1 = PAIRS[p]
        mm = jnp.where(lane[0:8, :] < 64, metar[origin(b0)], metar[origin(b1)])
        slot = ((((ii >> 4) + me) & 7) << 3) + (ii & 7) + 64 * zl
        slot = jnp.where(((ii >> 3) & 1) == (lane >> 6), slot, -1).astype(F32)
        hit0 = slot == mm[0:1, :]
        hit1 = slot == mm[1:2, :]
        sel = jnp.where(hit0 | hit1, 1.0, 0.0).astype(BF)
        for r, ref in ((2, whi), (3, wlo)):
            wt = jnp.where(hit0, mm[r:r + 1, :], 0.0) + jnp.where(hit1, mm[r + 2:r + 3, :], 0.0)
            ref[p] = jnp.transpose(wt).astype(BF)
        first = sbuf.at[g_me] if b0 == 0 else land.at[b0]

        @pl.loop(0, 4)
        def _(n):
            cols = pl.ds(pl.multiple_of(n * 512, 512), 512)
            rows = jnp.concatenate([first[:, cols], land[b1, :, cols]], axis=0)
            out = jnp.dot(sel, rows, preferred_element_type=F32).astype(BF)
            xbuf[p, :, cols] = out
            xin[p, 0:16, cols] = out[0:16, :]

        for o in (2, 6, 4, 5, 3, 7, 1):
            sl = pl.ds(16 * o, 16)
            mgo(xbuf.at[p, sl], xin.at[p, sl], 15 + p, xdev(me + o), note=False)

    rest = pl.ds(16, 112)

    def expert(p):
        mgot(xin.at[p, rest], 15 + p)
        rows = xin[p]
        gate_act = jnp.dot(rows, wg[...], preferred_element_type=F32)
        up_act = jnp.dot(rows, wu[...], preferred_element_type=F32)
        hidden = (gate_act / (1.0 + jnp.exp(-gate_act)) * up_act).astype(BF)

        @pl.loop(0, 4)
        def _(n):
            cols = pl.ds(pl.multiple_of(n * 512, 512), 512)
            out = jnp.dot(hidden, wd[:, cols], preferred_element_type=F32).astype(BF)
            pbuf[p, :, cols] = out
            rbuf[p, 0:16, cols] = out[0:16, :]

        for o in (2, 6, 4, 5, 3, 7, 1):
            sl = pl.ds(16 * o, 16)
            mgo(pbuf.at[p, sl], rbuf.at[p, sl], 19 + p, xdev(me - o), note=False)

    def merge(p):
        mgot(rbuf.at[p, rest], 19 + p)

        @pl.loop(0, 4)
        def _(n):
            cols = pl.ds(pl.multiple_of(n * 512, 512), 512)
            rows = rbuf[p, :, cols]
            out = (jnp.dot(whi[p], rows, preferred_element_type=F32)
                   + jnp.dot(wlo[p], rows, preferred_element_type=F32))
            for h, b in enumerate(PAIRS[p]):
                piece = out[64 * h:64 * (h + 1), :]
                if b < 4:
                    partk[b, :, cols] = piece
                else:
                    psend[b - 4, :, cols] = piece.astype(BF)

        for b in PAIRS[p]:
            if b >= 4:
                mgo(psend.at[b - 4], cback.at[b - 4], 19 + b, partner)

    def total(j):
        mgot(cback.at[j], 23 + j)

        @pl.loop(0, 4)
        def _(n):
            cols = pl.ds(pl.multiple_of(n * 512, 512), 512)
            out = (partk[j, :, cols] + cback[j, :, cols].astype(F32)).astype(BF)
            if j == 0:
                fin[g_me, :, cols] = out
            else:
                totb[j - 1, :, cols] = out

        if j:
            mgo(totb.at[j - 1], fin.at[g_me], 26 + j, zdev(z + sgn * j))

    for cp in loads:
        cp.wait()
    fwd(1)
    exchange(0)
    fwd(2)
    fwd(3)
    mgo(sbuf.at[g_me], land.at[4], 8, partner)
    exchange(1)
    expert(0)
    mgot(land.at[5], 12)
    mgot(land.at[6], 13)
    exchange(2)
    expert(1)
    merge(0)
    expert(2)
    merge(1)
    mgot(land.at[7], 14)
    mgot(land.at[4], 8)
    exchange(3)
    merge(2)
    expert(3)
    total(1)
    total(2)
    merge(3)
    total(3)
    total(0)
    for k in (1, 2, 3):
        mgot(fin.at[g_of[k]], 26 + k)

    @pl.loop(0, 8)
    def _(n):
        cols = pl.ds(pl.multiple_of(n * 256, 256), 256)
        out = stream[:, cols].astype(F32)
        rows = jnp.concatenate([fin[g, :, cols] for g in range(4)], axis=0)
        out += jnp.dot(pg_t[...], rows, preferred_element_type=F32)
        mixed_ref[:, cols] = out.astype(BF)

    for d in pending:
        d.wait_send()
    for p in range(4):
        mrc(xbuf.at[p, rest], xbuf.at[p, rest], 15 + p, partner).wait_send()
        mrc(pbuf.at[p, rest], pbuf.at[p, rest], 19 + p, partner).wait_send()


def layer(queries, key_rows, value_rows, doc_ids, sink_logit, residual, out_weight, norm_gain,
          gate_weight, up_weight, down_weight, routes, route_weights):
    vm = pl.BlockSpec(memory_space=pltpu.VMEM)
    anyspec = pl.BlockSpec(memory_space=pl.ANY)
    smem = pl.BlockSpec(memory_space=pltpu.SMEM)
    big = (4, 128, 2048)
    rows4 = (4, 64, 2048)
    dma = pltpu.SemaphoreType.DMA
    return pl.pallas_call(
        layer_kernel,
        out_shape=jax.ShapeDtypeStruct((256, 2048), BF),
        in_specs=[vm, vm, vm, vm, smem, vm, vm, vm] + [anyspec] * 5,
        out_specs=vm,
        scratch_shapes=[
            pltpu.VMEM((2, 1280, 128), BF),
            pltpu.VMEM((2, 1280, 256), BF),
            pltpu.VMEM((10, 1, 128), jnp.int32),
            pltpu.VMEM((2, 128, 128), BF),
            pltpu.VMEM((2, 128, 128), BF),
            pltpu.VMEM((3, 256, 512), BF),
            pltpu.VMEM((4, 256, 512), BF),
            pltpu.VMEM((3, 512, 2048), BF),
            pltpu.VMEM((512, 2048), BF),
            pltpu.VMEM((256, 2048), BF),
            pltpu.VMEM((256, 2048), F32),
            pltpu.VMEM((128, 384), F32),
            pltpu.VMEM((2, 512, 384), F32),
            pltpu.VMEM((2, 512, 384), BF),
            pltpu.VMEM((256, 128), F32),
            pltpu.VMEM((256, 2048), BF),
            pltpu.VMEM(rows4, BF),
            pltpu.VMEM((8, 64, 2048), BF),
            pltpu.VMEM((4, 8, 128), F32),
            pltpu.VMEM((8, 8, 128), F32),
            pltpu.VMEM((16, 256), F32),
            pltpu.VMEM((256, 256), BF),
            pltpu.VMEM((256, 256), BF),
            pltpu.VMEM((4, 128, 128), BF),
            pltpu.VMEM((4, 128, 128), BF),
            pltpu.VMEM(big, BF),
            pltpu.VMEM(big, BF),
            pltpu.VMEM(big, BF),
            pltpu.VMEM(big, BF),
            pltpu.VMEM(rows4, F32),
            pltpu.VMEM(rows4, BF),
            pltpu.VMEM(rows4, BF),
            pltpu.VMEM((3, 64, 2048), BF),
            pltpu.VMEM(rows4, BF),
            pltpu.VMEM((2048, 512), BF),
            pltpu.VMEM((2048, 512), BF),
            pltpu.VMEM((512, 2048), BF),
            dma((58,)), dma((58,)), dma((30,)), dma((30,)), dma((5,)),
        ],
        compiler_params=pltpu.CompilerParams(
            collective_id=0, has_side_effects=True, vmem_limit_bytes=62 * 2**20
        ),
        name="layer",
    )(
        queries, key_rows, value_rows, doc_ids.reshape(8, 1, 128), sink_logit,
        norm_gain.reshape(1, 2048), routes.T, route_weights.T, residual, out_weight,
        gate_weight, up_weight, down_weight,
    )


def per_device(
    queries,
    key_rows,
    value_rows,
    doc_ids,
    sink_logit,
    residual,
    out_weight,
    norm_gain,
    gate_weight,
    up_weight,
    down_weight,
    routes,
    route_weights,
):
    return layer(
        queries, key_rows, value_rows, doc_ids, sink_logit, residual, out_weight, norm_gain,
        gate_weight, up_weight, down_weight, routes, route_weights,
    )


def solution(mesh):
    return jax.shard_map(
        per_device,
        mesh=mesh,
        in_specs=(
            P("sp", "tp"),
            P("sp", "tp"),
            P("sp", "tp"),
            P("sp"),
            P("tp"),
            P(("sp", "tp"), None),
            P("tp", None),
            P(),
            P("sp", None, None),
            P("sp", None, None),
            P("sp", None, None),
            P(("sp", "tp"), None),
            P(("sp", "tp"), None),
        ),
        out_specs=P(("sp", "tp"), None),
        check_vma=False,
    )
```

```python
import jax
import jax.numpy as jnp
from jax import lax
from jax.experimental import pallas as pl
from jax.experimental.pallas import tpu as pltpu
from jax.sharding import PartitionSpec as P

HD = 64
BLK = 128
MESH = pl.DeviceIdType.MESH
NEG = -1e30
EPS = 1e-06
BF = jnp.bfloat16
F32 = jnp.float32


def coords():
    s = lax.axis_index("sp")
    y = lax.axis_index("tp")
    c = lax.rem(s, 2)
    x = lax.rem(s // 2, 4)
    z = s // 8
    return s, y, z, x, c


def sp_of(z, x, c):
    return (z * 4 + x) * 2 + c


PAIRS = ((0, 1), (2, 4), (6, 7), (3, 5))


def layer_kernel(
    q_ref, k_ref, v_ref, docs_ref, sink_ref, gain_ref, routes_ref, rw_ref,
    resid_hbm, w_hbm, gate_hbm, up_hbm, down_hbm,
    mixed_ref,
    k2, v3, dpad, khalo, vhalo, att, regr, wall, w_own, resid, acc, bias, scores, probs, squares,
    stream, sbuf, land, metas, metar, mscr, pg_n, pg_t, whi, wlo, xbuf, xin, pbuf, rbuf,
    partk, psend, cback, totb, fin, fin2, wg, wu, wd, fsend, frecv, msend, mrecv, lsem,
):
    s, y, z, x, c = coords()
    xm, xp = lax.rem(x + 3, 4), lax.rem(x + 1, 4)
    xo = lax.rem(x + 2, 4)
    me = 2 * x + c
    zl = lax.rem(z, 2)
    g_me = z // 2
    sgn = 2 * zl - 1

    def zdev(zz):
        return (sp_of(lax.rem(zz + 16, 8), x, c), y)

    def xdev(i):
        i = lax.rem(i + 8, 8)
        return (sp_of(z, i // 2, lax.rem(i, 2)), y)

    sp_next = (lax.rem(s + 1, 64), y)
    sp_prev = (lax.rem(s + 63, 64), y)
    sib = (sp_of(z, x, 1 - c), y)
    x_next = (sp_of(z, xp, c), y)
    x_prev = (sp_of(z, xm, c), y)
    z_next, z_prev = zdev(z + 1), zdev(z - 1)
    tps = [None] + [(s, lax.rem(y + r, 4)) for r in (1, 2, 3)]
    partner = zdev(z - sgn)

    def rc(src, dst, n, dev):
        return pltpu.make_async_remote_copy(
            src_ref=src, dst_ref=dst, send_sem=fsend.at[n], recv_sem=frecv.at[n],
            device_id=dev, device_id_type=MESH,
        )

    pending = []

    def go(src, dst, n, dev):
        d = rc(src, dst, n, dev)
        d.start()
        pending.append(d)

    def got(dst, n):
        rc(dst, dst, n, sib).wait_recv()


    def mrc(src, dst, n, dev):
        return pltpu.make_async_remote_copy(
            src_ref=src, dst_ref=dst, send_sem=msend.at[n], recv_sem=mrecv.at[n],
            device_id=dev, device_id_type=MESH,
        )

    def mgo(src, dst, n, dev, note=True):
        d = mrc(src, dst, n, dev)
        d.start()
        if note:
            pending.append(d)

    def mgot(dst, n):
        mrc(dst, dst, n, partner).wait_recv()

    w_copy = pltpu.make_async_copy(w_hbm, w_own, lsem.at[0])
    r_copy = pltpu.make_async_copy(resid_hbm, resid, lsem.at[1])
    w_copy.start()
    r_copy.start()
    loads = [pltpu.make_async_copy(a, b, lsem.at[2 + i])
             for i, (a, b) in enumerate(((gate_hbm.at[0], wg), (up_hbm.at[0], wu), (down_hbm.at[0], wd)))]
    for cp in loads:
        cp.start()
    barrier = pltpu.get_barrier_semaphore()
    greet = [sp_next, sp_prev, tps[1], tps[2], tps[3]]
    greet += [zdev(z + o) for o in range(1, 8)] + [xdev(me + o) for o in range(1, 8)]
    for dev in greet:
        pl.semaphore_signal(barrier, inc=1, device_id=dev, device_id_type=MESH)
    e0, e1 = routes_ref[0:1, :], routes_ref[1:2, :]
    upper = (lax.broadcasted_iota(jnp.int32, (256, 256), 0)
             < lax.broadcasted_iota(jnp.int32, (256, 256), 1)).astype(F32).astype(BF)
    ei = lax.broadcasted_iota(jnp.int32, (64, 256), 0)
    h0 = (ei == e0).astype(F32)
    h1 = (ei == e1).astype(F32)
    hg = (lax.broadcasted_iota(jnp.int32, (16, 256), 0) == (e0 >> 4)).astype(F32)

    def before(h):
        return jnp.dot(h.astype(BF), upper, preferred_element_type=F32)

    rank0 = jnp.sum(h0 * before(h0), axis=0, keepdims=True)
    rank1 = jnp.sum(h1 * (before(h1) + jnp.sum(h0, axis=1, keepdims=True)), axis=0, keepdims=True)
    gpos = jnp.sum(hg * before(hg), axis=0, keepdims=True) + ((e0 >> 4) * 64).astype(F32)
    w0, w1 = rw_ref[0:1, :], rw_ref[1:2, :]
    w0h = w0.astype(BF).astype(F32)
    w1h = w1.astype(BF).astype(F32)
    mscr[...] = jnp.zeros((16, 256), F32)
    mscr[0:1, :] = ((e0 & 15) * 8).astype(F32) + rank0
    mscr[1:2, :] = ((e1 & 15) * 8).astype(F32) + rank1
    mscr[2:3, :] = w0h
    mscr[3:4, :] = w0 - w0h
    mscr[4:5, :] = w1h
    mscr[5:6, :] = w1 - w1h
    pg = (lax.broadcasted_iota(jnp.int32, (256, 256), 0).astype(F32) == gpos).astype(F32)
    pg_t[...] = jnp.transpose(pg).astype(BF)
    pgb = pg.astype(BF)
    pg_n[...] = pgb
    info = mscr[...].astype(BF)
    for g in range(4):
        pgg = pgb[64 * g:64 * (g + 1), :]
        both = jnp.concatenate([pgg, pgg], axis=0)
        metas[g] = lax.dot_general(info, both, (((1,), (1,)), ((), ())),
                                   preferred_element_type=F32)[0:8, :]

    lane = lax.broadcasted_iota(jnp.int32, (BLK, BLK), 1)
    row = lax.broadcasted_iota(jnp.int32, (BLK, BLK), 0)
    low = lane < 64

    def dup(src, dst, at):
        v = src.astype(F32)
        rolled = pltpu.roll(v, 64, 1)
        dst[0, pl.ds(at, BLK), 0:BLK] = jnp.where(low, v, rolled).astype(BF)
        dst[1, pl.ds(at, BLK), 0:BLK] = jnp.where(low, rolled, v).astype(BF)

    @pl.loop(0, 8)
    def _(i):
        at = pl.multiple_of(i * BLK, BLK)
        dup(k_ref[pl.ds(at, BLK), :], k2, at + BLK)
        dup(v_ref[pl.ds(at, BLK), :], v3, at + BLK)
        dpad[i + 1] = docs_ref[i]

    @pl.loop(0, 10)
    def _(i):
        at = pl.multiple_of(i * BLK, BLK)
        for g in range(2):
            v3[g, pl.ds(at, BLK), BLK:2 * BLK] = jnp.ones((BLK, BLK), BF)

    pl.semaphore_wait(barrier, len(greet))

    go(k_ref.at[pl.ds(896, 128)], khalo.at[0], 0, sp_next)
    go(v_ref.at[pl.ds(896, 128)], vhalo.at[0], 1, sp_next)
    go(docs_ref.at[7], dpad.at[0], 2, sp_next)
    go(k_ref.at[pl.ds(0, 128)], khalo.at[1], 3, sp_prev)
    go(v_ref.at[pl.ds(0, 128)], vhalo.at[1], 4, sp_prev)
    go(docs_ref.at[0], dpad.at[9], 5, sp_prev)

    def rows_a(xx, cc, off, n):
        return pl.ds(pl.multiple_of(64 * xx + 32 * cc + off, 16), n)

    def rows_b(zz, cc):
        return pl.ds(pl.multiple_of(256 + 32 * lax.rem(zz + 16, 8) + 16 * cc, 16), 16)

    left, right = pl.ds(0, 1024), pl.ds(1024, 1024)
    w_copy.wait()
    mine = rows_a(x, c, 0, 32)
    mine_lo, mine_hi = rows_a(x, c, 0, 16), rows_a(x, c, 16, 16)
    mine_b = rows_b(z, c)
    go(w_own.at[mine], wall.at[0, mine], 6, tps[1])
    go(w_own.at[mine], wall.at[1, mine], 7, tps[3])
    go(w_own.at[mine_b], wall.at[0, mine_b], 30, tps[1])
    go(w_own.at[mine_b], wall.at[1, mine_b], 31, tps[3])

    for o in range(1, 8):
        zz = lax.rem(z + o, 8)
        mgo(metas.at[zz // 2], metar.at[o], o, zdev(z + o))
    metar[0] = metas[g_me]

    for n, ref in ((0, khalo.at[0]), (1, vhalo.at[0]), (2, dpad.at[0]),
                   (3, khalo.at[1]), (4, vhalo.at[1]), (5, dpad.at[9])):
        got(ref, n)
    dup(khalo[0], k2, 0)
    dup(khalo[1], k2, 9 * BLK)
    dup(vhalo[0], v3, 0)
    dup(vhalo[1], v3, 9 * BLK)
    dpad[0] = jnp.where(s == 0, -1, dpad[0])
    dpad[9] = jnp.where(s == 63, -1, dpad[9])

    scale = HD ** (-0.5)
    m_even = jnp.where(low, scale, 0.0).astype(BF)
    m_odd = jnp.where(low, 0.0, scale).astype(BF)

    def pair_of_blocks(t, out, out_at):
        p = lax.rem(y + 1 + t, 4)

        @pl.loop(0, 2)
        def _(sub):
            b = 2 * p + sub
            at = pl.multiple_of(b * BLK, BLK)
            qd = jnp.transpose(jnp.broadcast_to(dpad[b + 1].astype(F32), (BLK, BLK)))
            for j in range(3):
                ok = qd == dpad[b + j].astype(F32)
                if j == 0:
                    ok = ok & (lane >= row)
                if j == 2:
                    ok = ok & (lane <= row)
                bias[:, j * BLK:(j + 1) * BLK] = jnp.where(ok, 0.0, NEG)
            for g in range(2):
                keys = k2[g, pl.ds(at, 3 * BLK), :]
                qs = []
                for pair in range(2):
                    lo_col = g * 256 + pair * BLK
                    qq = q_ref[pl.ds(at, BLK), lo_col:lo_col + BLK]
                    qs += [qq * m_even, qq * m_odd]
                sc = lax.dot_general(jnp.concatenate(qs, axis=0), keys, (((1,), (1,)), ((), ())),
                                     preferred_element_type=F32)
                for h in range(4):
                    scores[g, h * BLK:(h + 1) * BLK, :] = sc[h * BLK:(h + 1) * BLK, :] + bias[...]
            extra = {}
            for g in range(2):
                for h in range(4):
                    sink = sink_ref[g * 4 + h]
                    sc = scores[g, h * BLK:(h + 1) * BLK, :]
                    top = jnp.maximum(jnp.max(sc, axis=1, keepdims=True), sink)
                    probs[g, h * BLK:(h + 1) * BLK, :] = jnp.exp(sc - top).astype(BF)
                    extra[g, h] = jnp.exp(sink - top)
            for g in range(2):
                o = jnp.dot(probs[g], v3[g, pl.ds(at, 3 * BLK), :], preferred_element_type=F32)
                for pair in range(2):
                    res = []
                    for half in range(2):
                        h = 2 * pair + half
                        oh = o[h * BLK:(h + 1) * BLK, :]
                        res.append(oh[:, 0:BLK] / (oh[:, BLK:2 * BLK] + extra[g, h]))
                    lo_col = g * 256 + pair * BLK
                    out[out_at, pl.ds(pl.multiple_of(sub * BLK, BLK), BLK), lo_col:lo_col + BLK] = (
                        jnp.where(low, res[0], res[1]).astype(BF))

    def send_att(t):
        r = t + 1
        go(att.at[t], regr.at[4 - r], 26 + t, tps[r])

    ab, dd = pl.ds(0, 2), pl.ds(2, 1)
    parts = (ab, dd)

    def zsend(step, sh):
        for d in range(2):
            zz = z - (step - 1) if d == 0 else z + (step - 1)
            rr = rows_b(zz, c)
            ref = wall.at[parts[sh], rr] if step < 4 else wall.at[parts[sh], rr, (left, right)[d]]
            go(ref, ref, 34 + (d * 2 + sh) * 4 + step - 1, (z_next, z_prev)[d])

    def zgot(step, sh):
        for d in range(2):
            zz = z - step if d == 0 else z + step
            rr = rows_b(zz, c)
            ref = wall.at[parts[sh], rr] if step < 4 else wall.at[parts[sh], rr, (left, right)[d]]
            got(ref, 34 + (d * 2 + sh) * 4 + step - 1)

    zorder = (0, -1, 1, -2, 2, -3, 3, 4)

    def zsib(sh, *dzs):
        for dz in dzs:
            ref = wall.at[parts[sh], rows_b(z + dz, c)]
            go(ref, ref, 68 + 2 * zorder.index(dz) + sh, sib)

    def xsib(sh, *ns):
        for n in ns:
            ref = wall.at[parts[sh], rows_a((x, xm, xp, xo)[n], c, 0, 32)]
            go(ref, ref, 60 + 2 * n + sh, sib)

    def sib_done(sh):
        for n, xx in enumerate((x, xm, xp, xo)):
            got(wall.at[parts[sh], rows_a(xx, 1 - c, 0, 32)], 60 + 2 * n + sh)
        for n, dz in enumerate(zorder):
            got(wall.at[parts[sh], rows_b(z + dz, 1 - c)], 68 + 2 * n + sh)

    from_m, from_p = rows_a(xm, c, 0, 32), rows_a(xp, c, 0, 32)
    fm_lo, fp_hi = rows_a(xm, c, 0, 16), rows_a(xp, c, 16, 16)
    far, far_lo, far_hi = rows_a(xo, c, 0, 32), rows_a(xo, c, 0, 16), rows_a(xo, c, 16, 16)

    def xsend(sh):
        ref = wall.at[parts[sh], mine]
        go(ref, ref, 10 + 2 * sh, x_next)
        go(ref, ref, 11 + 2 * sh, x_prev)

    def xforward(sh):
        got(wall.at[parts[sh], from_m], 10 + 2 * sh)
        got(wall.at[parts[sh], from_p], 11 + 2 * sh)
        ref = wall.at[parts[sh], fm_lo]
        go(ref, ref, 14 + 2 * sh, x_next)
        ref = wall.at[parts[sh], fp_hi]
        go(ref, ref, 15 + 2 * sh, x_prev)

    pair_of_blocks(0, att, 0)
    got(wall.at[0, mine], 6)
    go(wall.at[0, mine_lo], wall.at[2, mine_lo], 8, tps[1])
    got(wall.at[1, mine], 7)
    go(wall.at[1, mine_hi], wall.at[2, mine_hi], 9, tps[3])
    got(wall.at[0, mine_b], 30)
    go(wall.at[0, mine_b, left], wall.at[2, mine_b, left], 32, tps[1])
    got(wall.at[1, mine_b], 31)
    go(wall.at[1, mine_b, right], wall.at[2, mine_b, right], 33, tps[3])
    xsend(0)
    zsend(1, 0)
    pair_of_blocks(1, att, 1)
    send_att(0)
    got(wall.at[2, mine_lo], 8)
    got(wall.at[2, mine_hi], 9)
    got(wall.at[2, mine_b, left], 32)
    got(wall.at[2, mine_b, right], 33)
    xsend(1)
    zsend(1, 1)
    for sh in range(2):
        xsib(sh, 0)
        zsib(sh, 0)
    zgot(1, 0)
    zsend(2, 0)
    pair_of_blocks(2, att, 2)
    send_att(1)
    xforward(0)
    zgot(1, 1)
    zsend(2, 1)
    zgot(2, 0)
    zsend(3, 0)
    pair_of_blocks(3, regr, 0)
    send_att(2)
    xforward(1)
    zgot(2, 1)
    zsend(3, 1)
    zgot(3, 0)
    zsend(4, 0)
    for sh in range(2):
        xsib(sh, 1, 2)
        zsib(sh, -1, 1, -2, 2)
    zsib(0, -3, 3)

    r_copy.wait()

    def project(r, wref, first=False):
        @pl.loop(0, 4, unroll=True)
        def _(n):
            cols = pl.ds(pl.multiple_of(n * 512, 512), 512)
            part = jnp.dot(regr[r], wref[:, cols], preferred_element_type=F32)
            base = resid[:, cols].astype(F32) if first else acc[:, cols]
            acc[:, cols] = base + part.astype(BF).astype(F32)

    project(0, w_own, True)
    zgot(3, 1)
    zsend(4, 1)
    zsib(1, -3, 3)

    def last(sh):
        got(wall.at[parts[sh], far_lo], 14 + 2 * sh)
        got(wall.at[parts[sh], far_hi], 15 + 2 * sh)
        xsib(sh, 3)
        zgot(4, sh)
        zsib(sh, 4)

    last(0)
    last(1)
    sib_done(0)
    got(regr.at[1], 28)
    got(regr.at[3], 26)
    project(1, wall.at[1])
    project(3, wall.at[0])
    got(regr.at[2], 27)
    sib_done(1)
    squares[...] = jnp.zeros((256, BLK), F32)

    @pl.loop(0, 4, unroll=True)
    def _(n):
        cols = pl.ds(pl.multiple_of(n * 512, 512), 512)
        part = jnp.dot(regr[2], wall[2, :, cols], preferred_element_type=F32)
        st = (acc[:, cols] + part.astype(BF).astype(F32)).astype(BF)
        stream[:, cols] = st
        sq = st.astype(F32) * st.astype(F32)
        squares[...] += (sq[:, 0:128] + sq[:, 128:256]) + (sq[:, 256:384] + sq[:, 384:512])

    rms = lax.rsqrt(jnp.sum(squares[...], axis=1, keepdims=True) * (1.0 / 2048) + EPS)

    @pl.loop(0, 8, unroll=4)
    def _(n):
        cols = pl.ds(pl.multiple_of(n * 256, 256), 256)
        normed = (stream[:, cols].astype(F32) * rms * gain_ref[:, cols]).astype(BF)
        out = jnp.dot(pg_n[...], normed, preferred_element_type=F32).astype(BF)
        for g in range(4):
            sbuf[g, :, cols] = out[64 * g:64 * (g + 1), :]

    g_of = [g_me, lax.rem(g_me + sgn + 4, 4), lax.rem(g_me - sgn + 4, 4), lax.rem(g_me + 2, 4)]
    t_of = [None, z + sgn, z - 2 * sgn, z + 3 * sgn]
    mgo(sbuf.at[g_of[1]], land.at[1], 9, zdev(t_of[1]))
    mgo(sbuf.at[g_of[2]], land.at[2], 10, zdev(t_of[2]))
    mgo(sbuf.at[g_of[3]], land.at[3], 11, zdev(t_of[3]))
    mgo(sbuf.at[g_me], land.at[4], 8, partner)
    for o in range(1, 8):
        mgot(metar.at[o], o)

    def origin(b):
        if b == 0:
            return 0
        if b < 4:
            return lax.rem(8 - sgn * b, 8)
        return lax.rem(8 + sgn * (b - 3), 8)

    def fwd(k):
        mgo(land.at[k], land.at[4 + k], 11 + k, partner)

    ii = lax.broadcasted_iota(jnp.int32, (128, 128), 0)

    def exchange(p):
        b0, b1 = PAIRS[p]
        mm = jnp.where(lane[0:8, :] < 64, metar[origin(b0)], metar[origin(b1)])
        slot = ((((ii >> 4) + me) & 7) << 3) + (ii & 7) + 64 * zl
        slot = jnp.where(((ii >> 3) & 1) == (lane >> 6), slot, -1).astype(F32)
        hit0 = slot == mm[0:1, :]
        hit1 = slot == mm[1:2, :]
        sel = jnp.where(hit0 | hit1, 1.0, 0.0).astype(BF)
        for r, ref in ((2, whi), (3, wlo)):
            wt = jnp.where(hit0, mm[r:r + 1, :], 0.0) + jnp.where(hit1, mm[r + 2:r + 3, :], 0.0)
            ref[p] = jnp.transpose(wt).astype(BF)
        first = sbuf.at[g_me] if b0 == 0 else land.at[b0]

        @pl.loop(0, 4)
        def _(n):
            cols = pl.ds(pl.multiple_of(n * 512, 512), 512)
            rows = jnp.concatenate([first[:, cols], land[b1, :, cols]], axis=0)
            out = jnp.dot(sel, rows, preferred_element_type=F32).astype(BF)
            xbuf[p, :, cols] = out
            xin[p, 0:16, cols] = out[0:16, :]

        for o in (2, 6, 4, 5, 3, 7, 1):
            sl = pl.ds(16 * o, 16)
            mgo(xbuf.at[p, sl], xin.at[p, sl], 15 + p, xdev(me + o), note=False)

    rest = pl.ds(16, 112)
    half = (pl.ds(0, 1024), pl.ds(1024, 1024))

    def expert(p):
        mgot(xin.at[p, rest], 15 + p)
        rows = xin[p]
        gate_act = jnp.dot(rows, wg[...], preferred_element_type=F32)
        up_act = jnp.dot(rows, wu[...], preferred_element_type=F32)
        hidden = (gate_act / (1.0 + jnp.exp(-gate_act)) * up_act).astype(BF)

        for ch in range(2):
            @pl.loop(2 * ch, 2 * ch + 2, unroll=True)
            def _(n):
                cols = pl.ds(pl.multiple_of(n * 512, 512), 512)
                out = jnp.dot(hidden, wd[:, cols], preferred_element_type=F32).astype(BF)
                pbuf[p, :, cols] = out
                rbuf[p, 0:16, cols] = out[0:16, :]

            for o in (2, 6, 4, 5, 3, 7, 1):
                sl = pl.ds(16 * o, 16)
                mgo(pbuf.at[p, sl, half[ch]], rbuf.at[p, sl, half[ch]], 30 + 2 * p + ch, xdev(me - o), note=False)

    def merge(p, ch):
        hc = half[ch]
        mgot(rbuf.at[p, rest, hc], 30 + 2 * p + ch)

        @pl.loop(2 * ch, 2 * ch + 2, unroll=True)
        def _(n):
            cols = pl.ds(pl.multiple_of(n * 512, 512), 512)
            rows = rbuf[p, :, cols]
            out = (jnp.dot(whi[p], rows, preferred_element_type=F32)
                   + jnp.dot(wlo[p], rows, preferred_element_type=F32))
            for h, b in enumerate(PAIRS[p]):
                piece = out[64 * h:64 * (h + 1), :]
                if b == 0:
                    fin[g_me, :, cols] = piece.astype(BF)
                elif b == 1:
                    totb[0, :, cols] = piece.astype(BF)
                elif b < 4:
                    partk[b, :, cols] = piece
                else:
                    psend[b - 4, :, cols] = piece.astype(BF)

        for b in reversed(PAIRS[p]):
            n = 38 + 2 * (b - 4) + ch
            if b == 1:
                mgo(totb.at[0, :, hc], fin.at[g_me, :, hc], 46 + ch, zdev(z + sgn))
            elif b == 4:
                mgo(psend.at[0, :, hc], fin2.at[g_me, :, hc], n, partner)
            elif b == 5:
                mgo(psend.at[1, :, hc], fin2.at[g_me, :, hc], n, zdev(z - 2 * sgn))
            elif b > 5:
                mgo(psend.at[b - 4, :, hc], cback.at[b - 4, :, hc], n, partner)

    def total(j, ch):
        hc = half[ch]
        mgot(cback.at[j, :, hc], 38 + 2 * j + ch)
        totb[j - 1, :, hc] = (partk[j, :, hc] + cback[j, :, hc].astype(F32)).astype(BF)
        mgo(totb.at[j - 1, :, hc], fin.at[g_me, :, hc], 46 + 2 * (j - 1) + ch, zdev(z + sgn * j))

    for cp in loads:
        cp.wait()
    for k in (2, 3):
        fin2[g_of[k]] = jnp.zeros((64, 2048), BF)
    mgot(land.at[1], 9)
    exchange(0)
    mgot(land.at[2], 10)
    fwd(2)
    mgot(land.at[4], 8)
    exchange(1)
    expert(0)
    mgot(land.at[3], 11)
    fwd(3)
    fwd(1)
    expert(1)
    mgot(land.at[6], 13)
    mgot(land.at[7], 14)
    exchange(2)
    merge(0, 0)
    merge(0, 1)
    merge(1, 0)
    merge(1, 1)
    mgot(land.at[5], 12)
    exchange(3)
    expert(2)
    expert(3)
    merge(2, 0)
    merge(2, 1)
    merge(3, 0)
    total(3, 0)
    merge(3, 1)
    total(3, 1)
    total(2, 0)
    total(2, 1)
    for ch in range(2):
        hc = half[ch]
        mgot(fin2.at[g_me, :, hc], 38 + ch)
        mgot(fin2.at[g_of[1], :, hc], 40 + ch)
        for k in (1, 2, 3):
            mgot(fin.at[g_of[k], :, hc], 46 + 2 * (k - 1) + ch)

        @pl.loop(4 * ch, 4 * ch + 4, unroll=True)
        def _(n):
            cols = pl.ds(pl.multiple_of(n * 256, 256), 256)
            out = stream[:, cols].astype(F32)
            for ref in (fin, fin2):
                rows = jnp.concatenate([ref[g, :, cols] for g in range(4)], axis=0)
                out += jnp.dot(pg_t[...], rows, preferred_element_type=F32)
            mixed_ref[:, cols] = out.astype(BF)

    for d in pending:
        d.wait_send()
    for p in range(4):
        mrc(xbuf.at[p, rest], xbuf.at[p, rest], 15 + p, partner).wait_send()
        for ch in range(2):
            mrc(pbuf.at[p, rest, half[ch]], pbuf.at[p, rest, half[ch]], 30 + 2 * p + ch, partner).wait_send()


def layer(queries, key_rows, value_rows, doc_ids, sink_logit, residual, out_weight, norm_gain,
          gate_weight, up_weight, down_weight, routes, route_weights):
    vm = pl.BlockSpec(memory_space=pltpu.VMEM)
    anyspec = pl.BlockSpec(memory_space=pl.ANY)
    smem = pl.BlockSpec(memory_space=pltpu.SMEM)
    big = (4, 128, 2048)
    rows4 = (4, 64, 2048)
    dma = pltpu.SemaphoreType.DMA
    return pl.pallas_call(
        layer_kernel,
        out_shape=jax.ShapeDtypeStruct((256, 2048), BF),
        in_specs=[vm, vm, vm, vm, smem, vm, vm, vm] + [anyspec] * 5,
        out_specs=vm,
        scratch_shapes=[
            pltpu.VMEM((2, 1280, 128), BF),
            pltpu.VMEM((2, 1280, 256), BF),
            pltpu.VMEM((10, 1, 128), jnp.int32),
            pltpu.VMEM((2, 128, 128), BF),
            pltpu.VMEM((2, 128, 128), BF),
            pltpu.VMEM((3, 256, 512), BF),
            pltpu.VMEM((4, 256, 512), BF),
            pltpu.VMEM((3, 512, 2048), BF),
            pltpu.VMEM((512, 2048), BF),
            pltpu.VMEM((256, 2048), BF),
            pltpu.VMEM((256, 2048), F32),
            pltpu.VMEM((128, 384), F32),
            pltpu.VMEM((2, 512, 384), F32),
            pltpu.VMEM((2, 512, 384), BF),
            pltpu.VMEM((256, 128), F32),
            pltpu.VMEM((256, 2048), BF),
            pltpu.VMEM(rows4, BF),
            pltpu.VMEM((8, 64, 2048), BF),
            pltpu.VMEM((4, 8, 128), F32),
            pltpu.VMEM((8, 8, 128), F32),
            pltpu.VMEM((16, 256), F32),
            pltpu.VMEM((256, 256), BF),
            pltpu.VMEM((256, 256), BF),
            pltpu.VMEM((4, 128, 128), BF),
            pltpu.VMEM((4, 128, 128), BF),
            pltpu.VMEM(big, BF),
            pltpu.VMEM(big, BF),
            pltpu.VMEM(big, BF),
            pltpu.VMEM(big, BF),
            pltpu.VMEM(rows4, F32),
            pltpu.VMEM(rows4, BF),
            pltpu.VMEM(rows4, BF),
            pltpu.VMEM((3, 64, 2048), BF),
            pltpu.VMEM(rows4, BF),
            pltpu.VMEM(rows4, BF),
            pltpu.VMEM((2048, 512), BF),
            pltpu.VMEM((2048, 512), BF),
            pltpu.VMEM((512, 2048), BF),
            dma((84,)), dma((84,)), dma((52,)), dma((52,)), dma((5,)),
        ],
        compiler_params=pltpu.CompilerParams(
            collective_id=0, has_side_effects=True, vmem_limit_bytes=62 * 2**20
        ),
        name="layer",
    )(
        queries, key_rows, value_rows, doc_ids.reshape(8, 1, 128), sink_logit,
        norm_gain.reshape(1, 2048), routes.T, route_weights.T, residual, out_weight,
        gate_weight, up_weight, down_weight,
    )


def per_device(
    queries,
    key_rows,
    value_rows,
    doc_ids,
    sink_logit,
    residual,
    out_weight,
    norm_gain,
    gate_weight,
    up_weight,
    down_weight,
    routes,
    route_weights,
):
    return layer(
        queries, key_rows, value_rows, doc_ids, sink_logit, residual, out_weight, norm_gain,
        gate_weight, up_weight, down_weight, routes, route_weights,
    )


def solution(mesh):
    return jax.shard_map(
        per_device,
        mesh=mesh,
        in_specs=(
            P("sp", "tp"),
            P("sp", "tp"),
            P("sp", "tp"),
            P("sp"),
            P("tp"),
            P(("sp", "tp"), None),
            P("tp", None),
            P(),
            P("sp", None, None),
            P("sp", None, None),
            P("sp", None, None),
            P(("sp", "tp"), None),
            P(("sp", "tp"), None),
        ),
        out_specs=P(("sp", "tp"), None),
        check_vma=False,
    )
```

```python
import jax
import jax.numpy as jnp
from jax import lax
from jax.experimental import pallas as pl
from jax.experimental.pallas import tpu as pltpu
from jax.sharding import PartitionSpec as P

HD = 64
BLK = 128
MESH = pl.DeviceIdType.MESH
NEG = -1e30
EPS = 1e-06
BF = jnp.bfloat16
F32 = jnp.float32


def coords():
    s = lax.axis_index("sp")
    y = lax.axis_index("tp")
    c = lax.rem(s, 2)
    x = lax.rem(s // 2, 4)
    z = s // 8
    return s, y, z, x, c


def sp_of(z, x, c):
    return (z * 4 + x) * 2 + c


PAIRS = ((0, 1), (2, 4), (6, 7), (3, 5))


def layer_kernel(
    q_ref, k_ref, v_ref, docs_ref, sink_ref, gain_ref, routes_ref, rw_ref,
    resid_hbm, w_hbm, gate_hbm, up_hbm, down_hbm,
    mixed_ref,
    k2, v3, dpad, khalo, vhalo, att, regr, wall, w_own, resid, acc, bias, scores, probs, squares,
    stream, sbuf, land, metas, metar, mscr, pg_n, pg_t, whi, wlo, xbuf, xin, pbuf, rbuf,
    partk, psend, cback, totb, fin, fin2, wg, wu, wd, fsend, frecv, msend, mrecv, lsem,
):
    s, y, z, x, c = coords()
    xm, xp = lax.rem(x + 3, 4), lax.rem(x + 1, 4)
    xo = lax.rem(x + 2, 4)
    me = 2 * x + c
    zl = lax.rem(z, 2)
    g_me = z // 2
    sgn = 2 * zl - 1

    def zdev(zz):
        return (sp_of(lax.rem(zz + 16, 8), x, c), y)

    def xdev(i):
        i = lax.rem(i + 8, 8)
        return (sp_of(z, i // 2, lax.rem(i, 2)), y)

    sp_next = (lax.rem(s + 1, 64), y)
    sp_prev = (lax.rem(s + 63, 64), y)
    sib = (sp_of(z, x, 1 - c), y)
    x_next = (sp_of(z, xp, c), y)
    x_prev = (sp_of(z, xm, c), y)
    z_next, z_prev = zdev(z + 1), zdev(z - 1)
    tps = [None] + [(s, lax.rem(y + r, 4)) for r in (1, 2, 3)]
    partner = zdev(z - sgn)

    def rc(src, dst, n, dev):
        return pltpu.make_async_remote_copy(
            src_ref=src, dst_ref=dst, send_sem=fsend.at[n], recv_sem=frecv.at[n],
            device_id=dev, device_id_type=MESH,
        )

    pending = []

    def go(src, dst, n, dev):
        d = rc(src, dst, n, dev)
        d.start()
        pending.append(d)

    def got(dst, n):
        rc(dst, dst, n, sib).wait_recv()


    def mrc(src, dst, n, dev):
        return pltpu.make_async_remote_copy(
            src_ref=src, dst_ref=dst, send_sem=msend.at[n], recv_sem=mrecv.at[n],
            device_id=dev, device_id_type=MESH,
        )

    def mgo(src, dst, n, dev, note=True):
        d = mrc(src, dst, n, dev)
        d.start()
        if note:
            pending.append(d)

    def mgot(dst, n):
        mrc(dst, dst, n, partner).wait_recv()

    w_copy = pltpu.make_async_copy(w_hbm, w_own, lsem.at[0])
    r_copy = pltpu.make_async_copy(resid_hbm, resid, lsem.at[1])
    w_copy.start()
    r_copy.start()
    loads = [pltpu.make_async_copy(a, b, lsem.at[2 + i])
             for i, (a, b) in enumerate(((gate_hbm.at[0], wg), (up_hbm.at[0], wu), (down_hbm.at[0], wd)))]
    for cp in loads:
        cp.start()
    barrier = pltpu.get_barrier_semaphore()
    greet = [sp_next, sp_prev, tps[1], tps[2], tps[3]]
    greet += [zdev(z + o) for o in range(1, 8)] + [xdev(me + o) for o in range(1, 8)]
    for dev in greet:
        pl.semaphore_signal(barrier, inc=1, device_id=dev, device_id_type=MESH)
    e0, e1 = routes_ref[0:1, :], routes_ref[1:2, :]
    upper = (lax.broadcasted_iota(jnp.int32, (256, 256), 0)
             < lax.broadcasted_iota(jnp.int32, (256, 256), 1)).astype(F32).astype(BF)
    ei = lax.broadcasted_iota(jnp.int32, (64, 256), 0)
    h0 = (ei == e0).astype(F32)
    h1 = (ei == e1).astype(F32)
    hg = (lax.broadcasted_iota(jnp.int32, (16, 256), 0) == (e0 >> 4)).astype(F32)

    def before(h):
        return jnp.dot(h.astype(BF), upper, preferred_element_type=F32)

    rank0 = jnp.sum(h0 * before(h0), axis=0, keepdims=True)
    rank1 = jnp.sum(h1 * (before(h1) + jnp.sum(h0, axis=1, keepdims=True)), axis=0, keepdims=True)
    gpos = jnp.sum(hg * before(hg), axis=0, keepdims=True) + ((e0 >> 4) * 64).astype(F32)
    w0, w1 = rw_ref[0:1, :], rw_ref[1:2, :]
    w0h = w0.astype(BF).astype(F32)
    w1h = w1.astype(BF).astype(F32)
    mscr[...] = jnp.zeros((16, 256), F32)
    mscr[0:1, :] = ((e0 & 15) * 8).astype(F32) + rank0
    mscr[1:2, :] = ((e1 & 15) * 8).astype(F32) + rank1
    mscr[2:3, :] = w0h
    mscr[3:4, :] = w0 - w0h
    mscr[4:5, :] = w1h
    mscr[5:6, :] = w1 - w1h
    pg = (lax.broadcasted_iota(jnp.int32, (256, 256), 0).astype(F32) == gpos).astype(F32)
    pg_t[...] = jnp.transpose(pg).astype(BF)
    pgb = pg.astype(BF)
    pg_n[...] = pgb
    info = mscr[...].astype(BF)
    for g in range(4):
        pgg = pgb[64 * g:64 * (g + 1), :]
        both = jnp.concatenate([pgg, pgg], axis=0)
        metas[g] = lax.dot_general(info, both, (((1,), (1,)), ((), ())),
                                   preferred_element_type=F32)[0:8, :]

    lane = lax.broadcasted_iota(jnp.int32, (BLK, BLK), 1)
    row = lax.broadcasted_iota(jnp.int32, (BLK, BLK), 0)
    low = lane < 64

    def dup(src, dst, at):
        v = src.astype(F32)
        rolled = pltpu.roll(v, 64, 1)
        dst[0, pl.ds(at, BLK), 0:BLK] = jnp.where(low, v, rolled).astype(BF)
        dst[1, pl.ds(at, BLK), 0:BLK] = jnp.where(low, rolled, v).astype(BF)

    @pl.loop(0, 8)
    def _(i):
        at = pl.multiple_of(i * BLK, BLK)
        dup(k_ref[pl.ds(at, BLK), :], k2, at + BLK)
        dup(v_ref[pl.ds(at, BLK), :], v3, at + BLK)
        dpad[i + 1] = docs_ref[i]

    @pl.loop(0, 10)
    def _(i):
        at = pl.multiple_of(i * BLK, BLK)
        for g in range(2):
            v3[g, pl.ds(at, BLK), BLK:2 * BLK] = jnp.ones((BLK, BLK), BF)

    pl.semaphore_wait(barrier, len(greet))

    go(k_ref.at[pl.ds(896, 128)], khalo.at[0], 0, sp_next)
    go(v_ref.at[pl.ds(896, 128)], vhalo.at[0], 1, sp_next)
    go(docs_ref.at[7], dpad.at[0], 2, sp_next)
    go(k_ref.at[pl.ds(0, 128)], khalo.at[1], 3, sp_prev)
    go(v_ref.at[pl.ds(0, 128)], vhalo.at[1], 4, sp_prev)
    go(docs_ref.at[0], dpad.at[9], 5, sp_prev)

    def rows_a(xx, cc, off, n):
        return pl.ds(pl.multiple_of(64 * xx + 32 * cc + off, 16), n)

    def rows_b(zz, cc):
        return pl.ds(pl.multiple_of(256 + 32 * lax.rem(zz + 16, 8) + 16 * cc, 16), 16)

    left, right = pl.ds(0, 1024), pl.ds(1024, 1024)
    w_copy.wait()
    mine = rows_a(x, c, 0, 32)
    mine_lo, mine_hi = rows_a(x, c, 0, 16), rows_a(x, c, 16, 16)
    mine_b = rows_b(z, c)
    go(w_own.at[mine], wall.at[0, mine], 6, tps[1])
    go(w_own.at[mine], wall.at[1, mine], 7, tps[3])
    go(w_own.at[mine_b], wall.at[0, mine_b], 30, tps[1])
    go(w_own.at[mine_b], wall.at[1, mine_b], 31, tps[3])

    for o in range(1, 8):
        zz = lax.rem(z + o, 8)
        mgo(metas.at[zz // 2], metar.at[o], o, zdev(z + o))
    metar[0] = metas[g_me]

    for n, ref in ((0, khalo.at[0]), (1, vhalo.at[0]), (2, dpad.at[0]),
                   (3, khalo.at[1]), (4, vhalo.at[1]), (5, dpad.at[9])):
        got(ref, n)
    dup(khalo[0], k2, 0)
    dup(khalo[1], k2, 9 * BLK)
    dup(vhalo[0], v3, 0)
    dup(vhalo[1], v3, 9 * BLK)
    dpad[0] = jnp.where(s == 0, -1, dpad[0])
    dpad[9] = jnp.where(s == 63, -1, dpad[9])

    scale = HD ** (-0.5)
    m_even = jnp.where(low, scale, 0.0).astype(BF)
    m_odd = jnp.where(low, 0.0, scale).astype(BF)

    def pair_of_blocks(t, out, out_at):
        p = lax.rem(y + 1 + t, 4)

        @pl.loop(0, 2)
        def _(sub):
            b = 2 * p + sub
            at = pl.multiple_of(b * BLK, BLK)
            qd = jnp.transpose(jnp.broadcast_to(dpad[b + 1].astype(F32), (BLK, BLK)))
            for j in range(3):
                ok = qd == dpad[b + j].astype(F32)
                if j == 0:
                    ok = ok & (lane >= row)
                if j == 2:
                    ok = ok & (lane <= row)
                bias[:, j * BLK:(j + 1) * BLK] = jnp.where(ok, 0.0, NEG)
            for g in range(2):
                keys = k2[g, pl.ds(at, 3 * BLK), :]
                qs = []
                for pair in range(2):
                    lo_col = g * 256 + pair * BLK
                    qq = q_ref[pl.ds(at, BLK), lo_col:lo_col + BLK]
                    qs += [qq * m_even, qq * m_odd]
                sc = lax.dot_general(jnp.concatenate(qs, axis=0), keys, (((1,), (1,)), ((), ())),
                                     preferred_element_type=F32)
                for h in range(4):
                    scores[g, h * BLK:(h + 1) * BLK, :] = sc[h * BLK:(h + 1) * BLK, :] + bias[...]
            extra = {}
            for g in range(2):
                for h in range(4):
                    sink = sink_ref[g * 4 + h]
                    sc = scores[g, h * BLK:(h + 1) * BLK, :]
                    top = jnp.maximum(jnp.max(sc, axis=1, keepdims=True), sink)
                    probs[g, h * BLK:(h + 1) * BLK, :] = jnp.exp(sc - top).astype(BF)
                    extra[g, h] = jnp.exp(sink - top)
            for g in range(2):
                o = jnp.dot(probs[g], v3[g, pl.ds(at, 3 * BLK), :], preferred_element_type=F32)
                for pair in range(2):
                    res = []
                    for half in range(2):
                        h = 2 * pair + half
                        oh = o[h * BLK:(h + 1) * BLK, :]
                        res.append(oh[:, 0:BLK] / (oh[:, BLK:2 * BLK] + extra[g, h]))
                    lo_col = g * 256 + pair * BLK
                    out[out_at, pl.ds(pl.multiple_of(sub * BLK, BLK), BLK), lo_col:lo_col + BLK] = (
                        jnp.where(low, res[0], res[1]).astype(BF))

    def send_att(t):
        r = t + 1
        go(att.at[t], regr.at[4 - r], 26 + t, tps[r])

    ab, dd = pl.ds(0, 2), pl.ds(2, 1)
    parts = (ab, dd)

    def zsend(step, sh):
        for d in range(2):
            zz = z - (step - 1) if d == 0 else z + (step - 1)
            rr = rows_b(zz, c)
            ref = wall.at[parts[sh], rr] if step < 4 else wall.at[parts[sh], rr, (left, right)[d]]
            go(ref, ref, 34 + (d * 2 + sh) * 4 + step - 1, (z_next, z_prev)[d])

    def zgot(step, sh):
        for d in range(2):
            zz = z - step if d == 0 else z + step
            rr = rows_b(zz, c)
            ref = wall.at[parts[sh], rr] if step < 4 else wall.at[parts[sh], rr, (left, right)[d]]
            got(ref, 34 + (d * 2 + sh) * 4 + step - 1)

    zorder = (0, -1, 1, -2, 2, -3, 3, 4)

    def zsib(sh, *dzs):
        for dz in dzs:
            ref = wall.at[parts[sh], rows_b(z + dz, c)]
            go(ref, ref, 68 + 2 * zorder.index(dz) + sh, sib)

    def xsib(sh, *ns):
        for n in ns:
            ref = wall.at[parts[sh], rows_a((x, xm, xp, xo)[n], c, 0, 32)]
            go(ref, ref, 60 + 2 * n + sh, sib)

    def sib_done(sh):
        for n, xx in enumerate((x, xm, xp, xo)):
            got(wall.at[parts[sh], rows_a(xx, 1 - c, 0, 32)], 60 + 2 * n + sh)
        for n, dz in enumerate(zorder):
            got(wall.at[parts[sh], rows_b(z + dz, 1 - c)], 68 + 2 * n + sh)

    from_m, from_p = rows_a(xm, c, 0, 32), rows_a(xp, c, 0, 32)
    fm_lo, fp_hi = rows_a(xm, c, 0, 16), rows_a(xp, c, 16, 16)
    far, far_lo, far_hi = rows_a(xo, c, 0, 32), rows_a(xo, c, 0, 16), rows_a(xo, c, 16, 16)

    def xsend(sh):
        ref = wall.at[parts[sh], mine]
        go(ref, ref, 10 + 2 * sh, x_next)
        go(ref, ref, 11 + 2 * sh, x_prev)

    def xforward(sh):
        got(wall.at[parts[sh], from_m], 10 + 2 * sh)
        got(wall.at[parts[sh], from_p], 11 + 2 * sh)
        ref = wall.at[parts[sh], fm_lo]
        go(ref, ref, 14 + 2 * sh, x_next)
        ref = wall.at[parts[sh], fp_hi]
        go(ref, ref, 15 + 2 * sh, x_prev)

    pair_of_blocks(0, att, 0)
    got(wall.at[0, mine], 6)
    go(wall.at[0, mine_lo], wall.at[2, mine_lo], 8, tps[1])
    got(wall.at[1, mine], 7)
    go(wall.at[1, mine_hi], wall.at[2, mine_hi], 9, tps[3])
    got(wall.at[0, mine_b], 30)
    go(wall.at[0, mine_b, left], wall.at[2, mine_b, left], 32, tps[1])
    got(wall.at[1, mine_b], 31)
    go(wall.at[1, mine_b, right], wall.at[2, mine_b, right], 33, tps[3])
    xsend(0)
    zsend(1, 0)
    pair_of_blocks(1, att, 1)
    send_att(0)
    got(wall.at[2, mine_lo], 8)
    got(wall.at[2, mine_hi], 9)
    got(wall.at[2, mine_b, left], 32)
    got(wall.at[2, mine_b, right], 33)
    xsend(1)
    zsend(1, 1)
    for sh in range(2):
        xsib(sh, 0)
        zsib(sh, 0)
    zgot(1, 0)
    zsend(2, 0)
    pair_of_blocks(2, att, 2)
    send_att(1)
    xforward(0)
    zgot(1, 1)
    zsend(2, 1)
    zgot(2, 0)
    zsend(3, 0)
    pair_of_blocks(3, regr, 0)
    send_att(2)
    xforward(1)
    zgot(2, 1)
    zsend(3, 1)
    zgot(3, 0)
    zsend(4, 0)
    for sh in range(2):
        xsib(sh, 1, 2)
        zsib(sh, -1, 1, -2, 2)
    zsib(0, -3, 3)

    r_copy.wait()

    def project(r, wref, first=False):
        @pl.loop(0, 4, unroll=True)
        def _(n):
            cols = pl.ds(pl.multiple_of(n * 512, 512), 512)
            part = jnp.dot(regr[r], wref[:, cols], preferred_element_type=F32)
            base = resid[:, cols].astype(F32) if first else acc[:, cols]
            acc[:, cols] = base + part.astype(BF).astype(F32)

    project(0, w_own, True)
    zgot(3, 1)
    zsend(4, 1)
    zsib(1, -3, 3)

    def last(sh):
        got(wall.at[parts[sh], far_lo], 14 + 2 * sh)
        got(wall.at[parts[sh], far_hi], 15 + 2 * sh)
        xsib(sh, 3)
        zgot(4, sh)
        zsib(sh, 4)

    last(0)
    last(1)
    sib_done(0)
    got(regr.at[1], 28)
    got(regr.at[3], 26)
    project(1, wall.at[1])
    project(3, wall.at[0])
    got(regr.at[2], 27)
    sib_done(1)
    squares[...] = jnp.zeros((256, BLK), F32)

    @pl.loop(0, 4, unroll=True)
    def _(n):
        cols = pl.ds(pl.multiple_of(n * 512, 512), 512)
        part = jnp.dot(regr[2], wall[2, :, cols], preferred_element_type=F32)
        st = (acc[:, cols] + part.astype(BF).astype(F32)).astype(BF)
        stream[:, cols] = st
        sq = st.astype(F32) * st.astype(F32)
        squares[...] += (sq[:, 0:128] + sq[:, 128:256]) + (sq[:, 256:384] + sq[:, 384:512])

    rms = lax.rsqrt(jnp.sum(squares[...], axis=1, keepdims=True) * (1.0 / 2048) + EPS)

    half = (pl.ds(0, 1024), pl.ds(1024, 1024))
    g_of = [g_me, lax.rem(g_me + sgn + 4, 4), lax.rem(g_me - sgn + 4, 4), lax.rem(g_me + 2, 4)]
    t_of = [z - sgn, z + sgn, z - 2 * sgn, z + 3 * sgn]

    def zsem(b, ch):
        return 52 + 2 * (b - 1) + ch

    def depart(k, ch):
        hc = half[ch]
        b = k if k else 4
        mgo(sbuf.at[g_of[k], :, hc], land.at[b, :, hc], zsem(b, ch), zdev(t_of[k]))

    for ch in range(2):
        @pl.loop(4 * ch, 4 * ch + 4, unroll=True)
        def _(n):
            cols = pl.ds(pl.multiple_of(n * 256, 256), 256)
            normed = (stream[:, cols].astype(F32) * rms * gain_ref[:, cols]).astype(BF)
            out = jnp.dot(pg_n[...], normed, preferred_element_type=F32).astype(BF)
            for g in range(4):
                sbuf[g, :, cols] = out[64 * g:64 * (g + 1), :]

        depart(1, ch)
        depart(2, ch)
    for k in (3, 0):
        depart(k, 0)
        depart(k, 1)
    for o in range(1, 8):
        mgot(metar.at[o], o)

    def origin(b):
        if b == 0:
            return 0
        if b < 4:
            return lax.rem(8 - sgn * b, 8)
        return lax.rem(8 + sgn * (b - 3), 8)

    def arrive(b, ch):
        mgot(land.at[b, :, half[ch]], zsem(b, ch))

    def fwd(k, wait=True):
        for ch in range(2):
            if wait:
                arrive(k, ch)
            mgo(land.at[k, :, half[ch]], land.at[4 + k, :, half[ch]], zsem(4 + k, ch), partner)

    ii = lax.broadcasted_iota(jnp.int32, (128, 128), 0)

    def exchange(p, *waits):
        b0, b1 = PAIRS[p]
        mm = jnp.where(lane[0:8, :] < 64, metar[origin(b0)], metar[origin(b1)])
        slot = ((((ii >> 4) + me) & 7) << 3) + (ii & 7) + 64 * zl
        slot = jnp.where(((ii >> 3) & 1) == (lane >> 6), slot, -1).astype(F32)
        hit0 = slot == mm[0:1, :]
        hit1 = slot == mm[1:2, :]
        sel = jnp.where(hit0 | hit1, 1.0, 0.0).astype(BF)
        for r, ref in ((2, whi), (3, wlo)):
            wt = jnp.where(hit0, mm[r:r + 1, :], 0.0) + jnp.where(hit1, mm[r + 2:r + 3, :], 0.0)
            ref[p] = jnp.transpose(wt).astype(BF)
        first = sbuf.at[g_me] if b0 == 0 else land.at[b0]

        for ch in range(2):
            for b in waits:
                arrive(b, ch)

            @pl.loop(2 * ch, 2 * ch + 2, unroll=True)
            def _(n):
                cols = pl.ds(pl.multiple_of(n * 512, 512), 512)
                rows = jnp.concatenate([first[:, cols], land[b1, :, cols]], axis=0)
                out = jnp.dot(sel, rows, preferred_element_type=F32).astype(BF)
                xbuf[p, :, cols] = out
                xin[p, 0:16, cols] = out[0:16, :]

            for o in (4, 5, 3, 2, 6, 7, 1):
                sl = pl.ds(16 * o, 16)
                mgo(xbuf.at[p, sl, half[ch]], xin.at[p, sl, half[ch]], 66 + 2 * p + ch, xdev(me + o), note=False)

    rest = pl.ds(16, 112)

    def expert(p):
        gate_act = up_act = None
        for ch in range(2):
            hc = half[ch]
            mgot(xin.at[p, rest, hc], 66 + 2 * p + ch)
            rows = xin[p, :, hc]
            ga = jnp.dot(rows, wg[hc, :], preferred_element_type=F32)
            ua = jnp.dot(rows, wu[hc, :], preferred_element_type=F32)
            gate_act, up_act = (ga, ua) if ch == 0 else (gate_act + ga, up_act + ua)
        hidden = (gate_act / (1.0 + jnp.exp(-gate_act)) * up_act).astype(BF)

        for ch in range(2):
            @pl.loop(2 * ch, 2 * ch + 2, unroll=True)
            def _(n):
                cols = pl.ds(pl.multiple_of(n * 512, 512), 512)
                out = jnp.dot(hidden, wd[:, cols], preferred_element_type=F32).astype(BF)
                pbuf[p, :, cols] = out
                rbuf[p, 0:16, cols] = out[0:16, :]

            for o in (4, 5, 3, 2, 6, 7, 1):
                sl = pl.ds(16 * o, 16)
                mgo(pbuf.at[p, sl, half[ch]], rbuf.at[p, sl, half[ch]], 30 + 2 * p + ch, xdev(me - o), note=False)

    def merge(p, ch):
        hc = half[ch]
        mgot(rbuf.at[p, rest, hc], 30 + 2 * p + ch)

        @pl.loop(2 * ch, 2 * ch + 2, unroll=True)
        def _(n):
            cols = pl.ds(pl.multiple_of(n * 512, 512), 512)
            rows = rbuf[p, :, cols]
            out = (jnp.dot(whi[p], rows, preferred_element_type=F32)
                   + jnp.dot(wlo[p], rows, preferred_element_type=F32))
            for h, b in enumerate(PAIRS[p]):
                piece = out[64 * h:64 * (h + 1), :]
                if b == 0:
                    fin[g_me, :, cols] = piece.astype(BF)
                elif b == 1:
                    totb[0, :, cols] = piece.astype(BF)
                elif b < 4:
                    partk[b, :, cols] = piece
                else:
                    psend[b - 4, :, cols] = piece.astype(BF)

        for b in reversed(PAIRS[p]):
            n = 38 + 2 * (b - 4) + ch
            if b == 1:
                mgo(totb.at[0, :, hc], fin.at[g_me, :, hc], 46 + ch, zdev(z + sgn))
            elif b == 4:
                mgo(psend.at[0, :, hc], fin2.at[g_me, :, hc], n, partner)
            elif b == 5:
                mgo(psend.at[1, :, hc], fin2.at[g_me, :, hc], n, zdev(z - 2 * sgn))
            elif b > 5:
                mgo(psend.at[b - 4, :, hc], cback.at[b - 4, :, hc], n, partner)

    def total(j, ch):
        hc = half[ch]
        mgot(cback.at[j, :, hc], 38 + 2 * j + ch)
        totb[j - 1, :, hc] = (partk[j, :, hc] + cback[j, :, hc].astype(F32)).astype(BF)
        mgo(totb.at[j - 1, :, hc], fin.at[g_me, :, hc], 46 + 2 * (j - 1) + ch, zdev(z + sgn * j))

    for cp in loads:
        cp.wait()
    for k in (2, 3):
        fin2[g_of[k]] = jnp.zeros((64, 2048), BF)
    exchange(0, 1)
    fwd(2)
    exchange(1, 4)
    expert(0)
    fwd(3)
    fwd(1, False)
    expert(1)
    exchange(2, 6, 7)
    for p in (0, 1):
        merge(p, 0)
        merge(p, 1)
    exchange(3, 5)
    expert(2)
    merge(2, 0)
    expert(3)
    merge(2, 1)
    merge(3, 0)
    total(3, 0)
    total(2, 0)
    merge(3, 1)
    total(3, 1)
    total(2, 1)
    for ch in range(2):
        hc = half[ch]
        mgot(fin2.at[g_me, :, hc], 38 + ch)
        mgot(fin2.at[g_of[1], :, hc], 40 + ch)
        for k in (1, 2, 3):
            mgot(fin.at[g_of[k], :, hc], 46 + 2 * (k - 1) + ch)

        @pl.loop(4 * ch, 4 * ch + 4, unroll=True)
        def _(n):
            cols = pl.ds(pl.multiple_of(n * 256, 256), 256)
            out = stream[:, cols].astype(F32)
            for ref in (fin, fin2):
                rows = jnp.concatenate([ref[g, :, cols] for g in range(4)], axis=0)
                out += jnp.dot(pg_t[...], rows, preferred_element_type=F32)
            mixed_ref[:, cols] = out.astype(BF)

    for d in pending:
        d.wait_send()
    for p in range(4):
        for ch in range(2):
            mrc(xbuf.at[p, rest, half[ch]], xbuf.at[p, rest, half[ch]], 66 + 2 * p + ch, partner).wait_send()
            mrc(pbuf.at[p, rest, half[ch]], pbuf.at[p, rest, half[ch]], 30 + 2 * p + ch, partner).wait_send()


def layer(queries, key_rows, value_rows, doc_ids, sink_logit, residual, out_weight, norm_gain,
          gate_weight, up_weight, down_weight, routes, route_weights):
    vm = pl.BlockSpec(memory_space=pltpu.VMEM)
    anyspec = pl.BlockSpec(memory_space=pl.ANY)
    smem = pl.BlockSpec(memory_space=pltpu.SMEM)
    big = (4, 128, 2048)
    rows4 = (4, 64, 2048)
    dma = pltpu.SemaphoreType.DMA
    return pl.pallas_call(
        layer_kernel,
        out_shape=jax.ShapeDtypeStruct((256, 2048), BF),
        in_specs=[vm, vm, vm, vm, smem, vm, vm, vm] + [anyspec] * 5,
        out_specs=vm,
        scratch_shapes=[
            pltpu.VMEM((2, 1280, 128), BF),
            pltpu.VMEM((2, 1280, 256), BF),
            pltpu.VMEM((10, 1, 128), jnp.int32),
            pltpu.VMEM((2, 128, 128), BF),
            pltpu.VMEM((2, 128, 128), BF),
            pltpu.VMEM((3, 256, 512), BF),
            pltpu.VMEM((4, 256, 512), BF),
            pltpu.VMEM((3, 512, 2048), BF),
            pltpu.VMEM((512, 2048), BF),
            pltpu.VMEM((256, 2048), BF),
            pltpu.VMEM((256, 2048), F32),
            pltpu.VMEM((128, 384), F32),
            pltpu.VMEM((2, 512, 384), F32),
            pltpu.VMEM((2, 512, 384), BF),
            pltpu.VMEM((256, 128), F32),
            pltpu.VMEM((256, 2048), BF),
            pltpu.VMEM(rows4, BF),
            pltpu.VMEM((8, 64, 2048), BF),
            pltpu.VMEM((4, 8, 128), F32),
            pltpu.VMEM((8, 8, 128), F32),
            pltpu.VMEM((16, 256), F32),
            pltpu.VMEM((256, 256), BF),
            pltpu.VMEM((256, 256), BF),
            pltpu.VMEM((4, 128, 128), BF),
            pltpu.VMEM((4, 128, 128), BF),
            pltpu.VMEM(big, BF),
            pltpu.VMEM(big, BF),
            pltpu.VMEM(big, BF),
            pltpu.VMEM(big, BF),
            pltpu.VMEM(rows4, F32),
            pltpu.VMEM(rows4, BF),
            pltpu.VMEM(rows4, BF),
            pltpu.VMEM((3, 64, 2048), BF),
            pltpu.VMEM(rows4, BF),
            pltpu.VMEM(rows4, BF),
            pltpu.VMEM((2048, 512), BF),
            pltpu.VMEM((2048, 512), BF),
            pltpu.VMEM((512, 2048), BF),
            dma((84,)), dma((84,)), dma((74,)), dma((74,)), dma((5,)),
        ],
        compiler_params=pltpu.CompilerParams(
            collective_id=0, has_side_effects=True, vmem_limit_bytes=62 * 2**20
        ),
        name="layer",
    )(
        queries, key_rows, value_rows, doc_ids.reshape(8, 1, 128), sink_logit,
        norm_gain.reshape(1, 2048), routes.T, route_weights.T, residual, out_weight,
        gate_weight, up_weight, down_weight,
    )


def per_device(
    queries,
    key_rows,
    value_rows,
    doc_ids,
    sink_logit,
    residual,
    out_weight,
    norm_gain,
    gate_weight,
    up_weight,
    down_weight,
    routes,
    route_weights,
):
    return layer(
        queries, key_rows, value_rows, doc_ids, sink_logit, residual, out_weight, norm_gain,
        gate_weight, up_weight, down_weight, routes, route_weights,
    )


def solution(mesh):
    return jax.shard_map(
        per_device,
        mesh=mesh,
        in_specs=(
            P("sp", "tp"),
            P("sp", "tp"),
            P("sp", "tp"),
            P("sp"),
            P("tp"),
            P(("sp", "tp"), None),
            P("tp", None),
            P(),
            P("sp", None, None),
            P("sp", None, None),
            P("sp", None, None),
            P(("sp", "tp"), None),
            P(("sp", "tp"), None),
        ),
        out_specs=P(("sp", "tp"), None),
        check_vma=False,
    )
```

```python
import jax
import jax.numpy as jnp
from jax import lax
from jax.experimental import pallas as pl
from jax.experimental.pallas import tpu as pltpu
from jax.sharding import PartitionSpec as P

HD = 64
BLK = 128
MESH = pl.DeviceIdType.MESH
NEG = -1e30
EPS = 1e-06
BF = jnp.bfloat16
F32 = jnp.float32


def coords():
    s = lax.axis_index("sp")
    y = lax.axis_index("tp")
    c = lax.rem(s, 2)
    x = lax.rem(s // 2, 4)
    z = s // 8
    return s, y, z, x, c


def sp_of(z, x, c):
    return (z * 4 + x) * 2 + c


PAIRS = ((0, 1), (2, 4), (6, 7), (3, 5))


def layer_kernel(
    q_ref, k_ref, v_ref, docs_ref, sink_ref, gain_ref, routes_ref, rw_ref,
    resid_hbm, w_hbm, gate_hbm, up_hbm, down_hbm,
    mixed_ref,
    k2, v3, dpad, khalo, vhalo, att, regr, wall, w_own, resid, acc, bias, scores, probs, squares,
    stream, sbuf, land, metas, metar, mscr, pg_n, pg_t, whi, wlo, xbuf, xin, pbuf, rbuf,
    partk, psend, cback, totb, fin, fin2, wg, wu, wd, fsend, frecv, msend, mrecv, lsem,
):
    s, y, z, x, c = coords()
    xm, xp = lax.rem(x + 3, 4), lax.rem(x + 1, 4)
    xo = lax.rem(x + 2, 4)
    me = 2 * x + c
    zl = lax.rem(z, 2)
    g_me = z // 2
    sgn = 2 * zl - 1

    def zdev(zz):
        return (sp_of(lax.rem(zz + 16, 8), x, c), y)

    def xdev(i):
        i = lax.rem(i + 8, 8)
        return (sp_of(z, i // 2, lax.rem(i, 2)), y)

    sp_next = (lax.rem(s + 1, 64), y)
    sp_prev = (lax.rem(s + 63, 64), y)
    sib = (sp_of(z, x, 1 - c), y)
    x_next = (sp_of(z, xp, c), y)
    x_prev = (sp_of(z, xm, c), y)
    z_next, z_prev = zdev(z + 1), zdev(z - 1)
    tps = [None] + [(s, lax.rem(y + r, 4)) for r in (1, 2, 3)]
    partner = zdev(z - sgn)

    def rc(src, dst, n, dev):
        return pltpu.make_async_remote_copy(
            src_ref=src, dst_ref=dst, send_sem=fsend.at[n], recv_sem=frecv.at[n],
            device_id=dev, device_id_type=MESH,
        )

    pending = []

    def go(src, dst, n, dev):
        d = rc(src, dst, n, dev)
        d.start()
        pending.append(d)

    def got(dst, n):
        rc(dst, dst, n, sib).wait_recv()


    def mrc(src, dst, n, dev):
        return pltpu.make_async_remote_copy(
            src_ref=src, dst_ref=dst, send_sem=msend.at[n], recv_sem=mrecv.at[n],
            device_id=dev, device_id_type=MESH,
        )

    def mgo(src, dst, n, dev, note=True):
        d = mrc(src, dst, n, dev)
        d.start()
        if note:
            pending.append(d)

    def mgot(dst, n):
        mrc(dst, dst, n, partner).wait_recv()

    w_copy = pltpu.make_async_copy(w_hbm, w_own, lsem.at[0])
    r_copy = pltpu.make_async_copy(resid_hbm, resid, lsem.at[1])
    w_copy.start()
    r_copy.start()
    loads = [pltpu.make_async_copy(a, b, lsem.at[2 + i])
             for i, (a, b) in enumerate(((gate_hbm.at[0], wg), (up_hbm.at[0], wu), (down_hbm.at[0], wd)))]
    for cp in loads:
        cp.start()
    barrier = pltpu.get_barrier_semaphore()
    greet = [sp_next, sp_prev, tps[1], tps[2], tps[3]]
    greet += [zdev(z + o) for o in range(1, 8)] + [xdev(me + o) for o in range(1, 8)]
    for dev in greet:
        pl.semaphore_signal(barrier, inc=1, device_id=dev, device_id_type=MESH)
    e0, e1 = routes_ref[0:1, :], routes_ref[1:2, :]
    upper = (lax.broadcasted_iota(jnp.int32, (256, 256), 0)
             < lax.broadcasted_iota(jnp.int32, (256, 256), 1)).astype(F32).astype(BF)
    ei = lax.broadcasted_iota(jnp.int32, (64, 256), 0)
    h0 = (ei == e0).astype(F32)
    h1 = (ei == e1).astype(F32)
    hg = (lax.broadcasted_iota(jnp.int32, (16, 256), 0) == (e0 >> 4)).astype(F32)

    def before(h):
        return jnp.dot(h.astype(BF), upper, preferred_element_type=F32)

    rank0 = jnp.sum(h0 * before(h0), axis=0, keepdims=True)
    rank1 = jnp.sum(h1 * (before(h1) + jnp.sum(h0, axis=1, keepdims=True)), axis=0, keepdims=True)
    gpos = jnp.sum(hg * before(hg), axis=0, keepdims=True) + ((e0 >> 4) * 64).astype(F32)
    w0, w1 = rw_ref[0:1, :], rw_ref[1:2, :]
    w0h = w0.astype(BF).astype(F32)
    w1h = w1.astype(BF).astype(F32)
    mscr[...] = jnp.zeros((16, 256), F32)
    mscr[0:1, :] = ((e0 & 15) * 8).astype(F32) + rank0
    mscr[1:2, :] = ((e1 & 15) * 8).astype(F32) + rank1
    mscr[2:3, :] = w0h
    mscr[3:4, :] = w0 - w0h
    mscr[4:5, :] = w1h
    mscr[5:6, :] = w1 - w1h
    pg = (lax.broadcasted_iota(jnp.int32, (256, 256), 0).astype(F32) == gpos).astype(F32)
    pg_t[...] = jnp.transpose(pg).astype(BF)
    pgb = pg.astype(BF)
    pg_n[...] = pgb
    info = mscr[...].astype(BF)
    for g in range(4):
        pgg = pgb[64 * g:64 * (g + 1), :]
        both = jnp.concatenate([pgg, pgg], axis=0)
        metas[g] = lax.dot_general(info, both, (((1,), (1,)), ((), ())),
                                   preferred_element_type=F32)[0:8, :]

    lane = lax.broadcasted_iota(jnp.int32, (BLK, BLK), 1)
    row = lax.broadcasted_iota(jnp.int32, (BLK, BLK), 0)
    low = lane < 64

    def dup(src, dst, at):
        v = src.astype(F32)
        rolled = pltpu.roll(v, 64, 1)
        dst[0, pl.ds(at, BLK), 0:BLK] = jnp.where(low, v, rolled).astype(BF)
        dst[1, pl.ds(at, BLK), 0:BLK] = jnp.where(low, rolled, v).astype(BF)

    @pl.loop(0, 8)
    def _(i):
        at = pl.multiple_of(i * BLK, BLK)
        dup(k_ref[pl.ds(at, BLK), :], k2, at + BLK)
        dup(v_ref[pl.ds(at, BLK), :], v3, at + BLK)
        dpad[i + 1] = docs_ref[i]

    @pl.loop(0, 10)
    def _(i):
        at = pl.multiple_of(i * BLK, BLK)
        for g in range(2):
            v3[g, pl.ds(at, BLK), BLK:2 * BLK] = jnp.ones((BLK, BLK), BF)

    pl.semaphore_wait(barrier, len(greet))

    go(k_ref.at[pl.ds(896, 128)], khalo.at[0], 0, sp_next)
    go(v_ref.at[pl.ds(896, 128)], vhalo.at[0], 1, sp_next)
    go(docs_ref.at[7], dpad.at[0], 2, sp_next)
    go(k_ref.at[pl.ds(0, 128)], khalo.at[1], 3, sp_prev)
    go(v_ref.at[pl.ds(0, 128)], vhalo.at[1], 4, sp_prev)
    go(docs_ref.at[0], dpad.at[9], 5, sp_prev)

    def rows_a(xx, cc, off, n):
        return pl.ds(pl.multiple_of(64 * xx + 32 * cc + off, 16), n)

    def rows_b(zz, cc):
        return pl.ds(pl.multiple_of(256 + 32 * lax.rem(zz + 16, 8) + 16 * cc, 16), 16)

    left, right = pl.ds(0, 1024), pl.ds(1024, 1024)
    w_copy.wait()
    mine = rows_a(x, c, 0, 32)
    mine_lo, mine_hi = rows_a(x, c, 0, 16), rows_a(x, c, 16, 16)
    mine_b = rows_b(z, c)
    go(w_own.at[mine_b], wall.at[0, mine_b], 30, tps[1])
    go(w_own.at[mine_b], wall.at[1, mine_b], 31, tps[3])
    go(w_own.at[mine], wall.at[0, mine], 6, tps[1])
    go(w_own.at[mine], wall.at[1, mine], 7, tps[3])

    for o in range(1, 8):
        zz = lax.rem(z + o, 8)
        mgo(metas.at[zz // 2], metar.at[o], o, zdev(z + o))
    metar[0] = metas[g_me]

    for n, ref in ((0, khalo.at[0]), (1, vhalo.at[0]), (2, dpad.at[0]),
                   (3, khalo.at[1]), (4, vhalo.at[1]), (5, dpad.at[9])):
        got(ref, n)
    dup(khalo[0], k2, 0)
    dup(khalo[1], k2, 9 * BLK)
    dup(vhalo[0], v3, 0)
    dup(vhalo[1], v3, 9 * BLK)
    dpad[0] = jnp.where(s == 0, -1, dpad[0])
    dpad[9] = jnp.where(s == 63, -1, dpad[9])

    scale = HD ** (-0.5)
    m_even = jnp.where(low, scale, 0.0).astype(BF)
    m_odd = jnp.where(low, 0.0, scale).astype(BF)

    def pair_of_blocks(t, out, out_at):
        p = lax.rem(y + 1 + t, 4)

        @pl.loop(0, 2)
        def _(sub):
            b = 2 * p + sub
            at = pl.multiple_of(b * BLK, BLK)
            qd = jnp.transpose(jnp.broadcast_to(dpad[b + 1].astype(F32), (BLK, BLK)))
            for j in range(3):
                ok = qd == dpad[b + j].astype(F32)
                if j == 0:
                    ok = ok & (lane >= row)
                if j == 2:
                    ok = ok & (lane <= row)
                bias[:, j * BLK:(j + 1) * BLK] = jnp.where(ok, 0.0, NEG)
            for g in range(2):
                keys = k2[g, pl.ds(at, 3 * BLK), :]
                qs = []
                for pair in range(2):
                    lo_col = g * 256 + pair * BLK
                    qq = q_ref[pl.ds(at, BLK), lo_col:lo_col + BLK]
                    qs += [qq * m_even, qq * m_odd]
                sc = lax.dot_general(jnp.concatenate(qs, axis=0), keys, (((1,), (1,)), ((), ())),
                                     preferred_element_type=F32)
                for h in range(4):
                    scores[g, h * BLK:(h + 1) * BLK, :] = sc[h * BLK:(h + 1) * BLK, :] + bias[...]
            extra = {}
            for g in range(2):
                for h in range(4):
                    sink = sink_ref[g * 4 + h]
                    sc = scores[g, h * BLK:(h + 1) * BLK, :]
                    top = jnp.maximum(jnp.max(sc, axis=1, keepdims=True), sink)
                    probs[g, h * BLK:(h + 1) * BLK, :] = jnp.exp(sc - top).astype(BF)
                    extra[g, h] = jnp.exp(sink - top)
            for g in range(2):
                o = jnp.dot(probs[g], v3[g, pl.ds(at, 3 * BLK), :], preferred_element_type=F32)
                for pair in range(2):
                    res = []
                    for half in range(2):
                        h = 2 * pair + half
                        oh = o[h * BLK:(h + 1) * BLK, :]
                        res.append(oh[:, 0:BLK] / (oh[:, BLK:2 * BLK] + extra[g, h]))
                    lo_col = g * 256 + pair * BLK
                    out[out_at, pl.ds(pl.multiple_of(sub * BLK, BLK), BLK), lo_col:lo_col + BLK] = (
                        jnp.where(low, res[0], res[1]).astype(BF))

    def send_att(t):
        r = t + 1
        go(att.at[t], regr.at[4 - r], 26 + t, tps[r])

    ab, dd = pl.ds(0, 2), pl.ds(2, 1)
    parts = (ab, dd)

    def zsend(step, sh):
        for d in range(2):
            zz = z - (step - 1) if d == 0 else z + (step - 1)
            rr = rows_b(zz, c)
            ref = wall.at[parts[sh], rr] if step < 4 else wall.at[parts[sh], rr, (left, right)[d]]
            go(ref, ref, 34 + (d * 2 + sh) * 4 + step - 1, (z_next, z_prev)[d])

    def zgot(step, sh):
        for d in range(2):
            zz = z - step if d == 0 else z + step
            rr = rows_b(zz, c)
            ref = wall.at[parts[sh], rr] if step < 4 else wall.at[parts[sh], rr, (left, right)[d]]
            got(ref, 34 + (d * 2 + sh) * 4 + step - 1)

    zorder = (0, -1, 1, -2, 2, -3, 3, 4)

    def zsib(sh, *dzs):
        for dz in dzs:
            ref = wall.at[parts[sh], rows_b(z + dz, c)]
            go(ref, ref, 68 + 2 * zorder.index(dz) + sh, sib)

    def xsib(sh, *ns):
        for n in ns:
            ref = wall.at[parts[sh], rows_a((x, xm, xp, xo)[n], c, 0, 32)]
            go(ref, ref, 60 + 2 * n + sh, sib)

    def sib_done(sh):
        for n, xx in enumerate((x, xm, xp, xo)):
            got(wall.at[parts[sh], rows_a(xx, 1 - c, 0, 32)], 60 + 2 * n + sh)
        for n, dz in enumerate(zorder):
            got(wall.at[parts[sh], rows_b(z + dz, 1 - c)], 68 + 2 * n + sh)

    from_m, from_p = rows_a(xm, c, 0, 32), rows_a(xp, c, 0, 32)
    fm_lo, fp_hi = rows_a(xm, c, 0, 16), rows_a(xp, c, 16, 16)
    far, far_lo, far_hi = rows_a(xo, c, 0, 32), rows_a(xo, c, 0, 16), rows_a(xo, c, 16, 16)

    def xsend(sh):
        ref = wall.at[parts[sh], mine]
        go(ref, ref, 10 + 2 * sh, x_next)
        go(ref, ref, 11 + 2 * sh, x_prev)

    def xforward(sh):
        got(wall.at[parts[sh], from_m], 10 + 2 * sh)
        got(wall.at[parts[sh], from_p], 11 + 2 * sh)
        ref = wall.at[parts[sh], fm_lo]
        go(ref, ref, 14 + 2 * sh, x_next)
        ref = wall.at[parts[sh], fp_hi]
        go(ref, ref, 15 + 2 * sh, x_prev)

    pair_of_blocks(0, att, 0)
    got(wall.at[0, mine_b], 30)
    go(wall.at[0, mine_b, left], wall.at[2, mine_b, left], 32, tps[1])
    got(wall.at[1, mine_b], 31)
    go(wall.at[1, mine_b, right], wall.at[2, mine_b, right], 33, tps[3])
    zsend(1, 0)
    got(wall.at[0, mine], 6)
    go(wall.at[0, mine_lo], wall.at[2, mine_lo], 8, tps[1])
    got(wall.at[1, mine], 7)
    go(wall.at[1, mine_hi], wall.at[2, mine_hi], 9, tps[3])
    xsend(0)
    pair_of_blocks(1, att, 1)
    send_att(0)
    got(wall.at[2, mine_b, left], 32)
    got(wall.at[2, mine_b, right], 33)
    zsend(1, 1)
    zgot(1, 0)
    zsend(2, 0)
    got(wall.at[2, mine_lo], 8)
    got(wall.at[2, mine_hi], 9)
    xsend(1)
    for sh in range(2):
        xsib(sh, 0)
        zsib(sh, 0)
    pair_of_blocks(2, att, 2)
    send_att(1)
    zgot(1, 1)
    zsend(2, 1)
    zgot(2, 0)
    zsend(3, 0)
    xforward(0)
    pair_of_blocks(3, regr, 0)
    send_att(2)
    zgot(2, 1)
    zsend(3, 1)
    zgot(3, 0)
    zsend(4, 0)
    xforward(1)
    for sh in range(2):
        xsib(sh, 1, 2)
        zsib(sh, -1, 1, -2, 2)
    zsib(0, -3, 3)

    r_copy.wait()

    def project(r, wref, first=False):
        @pl.loop(0, 4, unroll=True)
        def _(n):
            cols = pl.ds(pl.multiple_of(n * 512, 512), 512)
            part = jnp.dot(regr[r], wref[:, cols], preferred_element_type=F32)
            base = resid[:, cols].astype(F32) if first else acc[:, cols]
            acc[:, cols] = base + part.astype(BF).astype(F32)

    project(0, w_own, True)
    zgot(3, 1)
    zsend(4, 1)
    zsib(1, -3, 3)

    def last(sh):
        got(wall.at[parts[sh], far_lo], 14 + 2 * sh)
        got(wall.at[parts[sh], far_hi], 15 + 2 * sh)
        xsib(sh, 3)
        zgot(4, sh)
        zsib(sh, 4)

    last(0)
    last(1)
    sib_done(0)
    got(regr.at[1], 28)
    got(regr.at[3], 26)
    project(1, wall.at[1])
    project(3, wall.at[0])
    got(regr.at[2], 27)
    sib_done(1)
    squares[...] = jnp.zeros((256, BLK), F32)

    @pl.loop(0, 4, unroll=True)
    def _(n):
        cols = pl.ds(pl.multiple_of(n * 512, 512), 512)
        part = jnp.dot(regr[2], wall[2, :, cols], preferred_element_type=F32)
        st = (acc[:, cols] + part.astype(BF).astype(F32)).astype(BF)
        stream[:, cols] = st
        sq = st.astype(F32) * st.astype(F32)
        squares[...] += (sq[:, 0:128] + sq[:, 128:256]) + (sq[:, 256:384] + sq[:, 384:512])

    rms = lax.rsqrt(jnp.sum(squares[...], axis=1, keepdims=True) * (1.0 / 2048) + EPS)

    half = (pl.ds(0, 1024), pl.ds(1024, 1024))
    g_of = [g_me, lax.rem(g_me + sgn + 4, 4), lax.rem(g_me - sgn + 4, 4), lax.rem(g_me + 2, 4)]
    t_of = [z - sgn, z + sgn, z - 2 * sgn, z + 3 * sgn]

    def zsem(b, ch):
        return 52 + 2 * (b - 1) + ch

    def depart(k, ch):
        hc = half[ch]
        b = k if k else 4
        mgo(sbuf.at[g_of[k], :, hc], land.at[b, :, hc], zsem(b, ch), zdev(t_of[k]))

    for ch in range(2):
        @pl.loop(4 * ch, 4 * ch + 4, unroll=True)
        def _(n):
            cols = pl.ds(pl.multiple_of(n * 256, 256), 256)
            normed = (stream[:, cols].astype(F32) * rms * gain_ref[:, cols]).astype(BF)
            out = jnp.dot(pg_n[...], normed, preferred_element_type=F32).astype(BF)
            for g in range(4):
                sbuf[g, :, cols] = out[64 * g:64 * (g + 1), :]

        depart(1, ch)
        depart(2, ch)
    for k in (3, 0):
        depart(k, 0)
        depart(k, 1)
    for o in range(1, 8):
        mgot(metar.at[o], o)

    def origin(b):
        if b == 0:
            return 0
        if b < 4:
            return lax.rem(8 - sgn * b, 8)
        return lax.rem(8 + sgn * (b - 3), 8)

    def arrive(b, ch):
        mgot(land.at[b, :, half[ch]], zsem(b, ch))

    def fwd(k, wait=True):
        for ch in range(2):
            if wait:
                arrive(k, ch)
            mgo(land.at[k, :, half[ch]], land.at[4 + k, :, half[ch]], zsem(4 + k, ch), partner)

    ii = lax.broadcasted_iota(jnp.int32, (128, 128), 0)

    def exchange(p, *waits):
        b0, b1 = PAIRS[p]
        mm = jnp.where(lane[0:8, :] < 64, metar[origin(b0)], metar[origin(b1)])
        slot = ((((ii >> 4) + me) & 7) << 3) + (ii & 7) + 64 * zl
        slot = jnp.where(((ii >> 3) & 1) == (lane >> 6), slot, -1).astype(F32)
        hit0 = slot == mm[0:1, :]
        hit1 = slot == mm[1:2, :]
        sel = jnp.where(hit0 | hit1, 1.0, 0.0).astype(BF)
        for r, ref in ((2, whi), (3, wlo)):
            wt = jnp.where(hit0, mm[r:r + 1, :], 0.0) + jnp.where(hit1, mm[r + 2:r + 3, :], 0.0)
            ref[p] = jnp.transpose(wt).astype(BF)
        first = sbuf.at[g_me] if b0 == 0 else land.at[b0]

        for ch in range(2):
            for b in waits:
                arrive(b, ch)

            @pl.loop(2 * ch, 2 * ch + 2, unroll=True)
            def _(n):
                cols = pl.ds(pl.multiple_of(n * 512, 512), 512)
                rows = jnp.concatenate([first[:, cols], land[b1, :, cols]], axis=0)
                out = jnp.dot(sel, rows, preferred_element_type=F32).astype(BF)
                xbuf[p, :, cols] = out
                xin[p, 0:16, cols] = out[0:16, :]

            for o in (4, 5, 3, 2, 6, 7, 1):
                sl = pl.ds(16 * o, 16)
                mgo(xbuf.at[p, sl, half[ch]], xin.at[p, sl, half[ch]], 66 + 2 * p + ch, xdev(me + o), note=False)

    rest = pl.ds(16, 112)

    def expert(p):
        gate_act = up_act = None
        for ch in range(2):
            hc = half[ch]
            mgot(xin.at[p, rest, hc], 66 + 2 * p + ch)
            rows = xin[p, :, hc]
            ga = jnp.dot(rows, wg[hc, :], preferred_element_type=F32)
            ua = jnp.dot(rows, wu[hc, :], preferred_element_type=F32)
            gate_act, up_act = (ga, ua) if ch == 0 else (gate_act + ga, up_act + ua)
        hidden = (gate_act / (1.0 + jnp.exp(-gate_act)) * up_act).astype(BF)

        for ch in range(2):
            @pl.loop(2 * ch, 2 * ch + 2, unroll=True)
            def _(n):
                cols = pl.ds(pl.multiple_of(n * 512, 512), 512)
                out = jnp.dot(hidden, wd[:, cols], preferred_element_type=F32).astype(BF)
                pbuf[p, :, cols] = out
                rbuf[p, 0:16, cols] = out[0:16, :]

            for o in (4, 5, 3, 2, 6, 7, 1):
                sl = pl.ds(16 * o, 16)
                mgo(pbuf.at[p, sl, half[ch]], rbuf.at[p, sl, half[ch]], 30 + 2 * p + ch, xdev(me - o), note=False)

    def merge(p, ch):
        hc = half[ch]
        mgot(rbuf.at[p, rest, hc], 30 + 2 * p + ch)

        @pl.loop(2 * ch, 2 * ch + 2, unroll=True)
        def _(n):
            cols = pl.ds(pl.multiple_of(n * 512, 512), 512)
            rows = rbuf[p, :, cols]
            out = (jnp.dot(whi[p], rows, preferred_element_type=F32)
                   + jnp.dot(wlo[p], rows, preferred_element_type=F32))
            for h, b in enumerate(PAIRS[p]):
                piece = out[64 * h:64 * (h + 1), :]
                if b == 0:
                    fin[g_me, :, cols] = piece.astype(BF)
                elif b == 1:
                    totb[0, :, cols] = piece.astype(BF)
                elif b < 4:
                    partk[b, :, cols] = piece
                else:
                    psend[b - 4, :, cols] = piece.astype(BF)

        for b in reversed(PAIRS[p]):
            n = 38 + 2 * (b - 4) + ch
            if b == 1:
                mgo(totb.at[0, :, hc], fin.at[g_me, :, hc], 46 + ch, zdev(z + sgn))
            elif b == 4:
                mgo(psend.at[0, :, hc], fin2.at[g_me, :, hc], n, partner)
            elif b == 5:
                mgo(psend.at[1, :, hc], fin2.at[g_me, :, hc], n, zdev(z - 2 * sgn))
            elif b > 5:
                mgo(psend.at[b - 4, :, hc], cback.at[b - 4, :, hc], n, partner)

    def total(j, ch):
        hc = half[ch]
        mgot(cback.at[j, :, hc], 38 + 2 * j + ch)
        totb[j - 1, :, hc] = (partk[j, :, hc] + cback[j, :, hc].astype(F32)).astype(BF)
        mgo(totb.at[j - 1, :, hc], fin.at[g_me, :, hc], 46 + 2 * (j - 1) + ch, zdev(z + sgn * j))

    for cp in loads:
        cp.wait()
    for k in (2, 3):
        fin2[g_of[k]] = jnp.zeros((64, 2048), BF)
    exchange(0, 1)
    fwd(2)
    exchange(1, 4)
    expert(0)
    fwd(3)
    fwd(1, False)
    expert(1)
    exchange(2, 6, 7)
    for p in (0, 1):
        merge(p, 0)
        merge(p, 1)
    exchange(3, 5)
    expert(2)
    merge(2, 0)
    expert(3)
    merge(2, 1)
    merge(3, 0)
    total(3, 0)
    total(2, 0)
    merge(3, 1)
    total(3, 1)
    total(2, 1)
    for ch in range(2):
        hc = half[ch]
        mgot(fin2.at[g_me, :, hc], 38 + ch)
        mgot(fin2.at[g_of[1], :, hc], 40 + ch)
        for k in (1, 2, 3):
            mgot(fin.at[g_of[k], :, hc], 46 + 2 * (k - 1) + ch)

        @pl.loop(4 * ch, 4 * ch + 4, unroll=True)
        def _(n):
            cols = pl.ds(pl.multiple_of(n * 256, 256), 256)
            out = stream[:, cols].astype(F32)
            for ref in (fin, fin2):
                rows = jnp.concatenate([ref[g, :, cols] for g in range(4)], axis=0)
                out += jnp.dot(pg_t[...], rows, preferred_element_type=F32)
            mixed_ref[:, cols] = out.astype(BF)

    for d in pending:
        d.wait_send()
    for p in range(4):
        for ch in range(2):
            mrc(xbuf.at[p, rest, half[ch]], xbuf.at[p, rest, half[ch]], 66 + 2 * p + ch, partner).wait_send()
            mrc(pbuf.at[p, rest, half[ch]], pbuf.at[p, rest, half[ch]], 30 + 2 * p + ch, partner).wait_send()


def layer(queries, key_rows, value_rows, doc_ids, sink_logit, residual, out_weight, norm_gain,
          gate_weight, up_weight, down_weight, routes, route_weights):
    vm = pl.BlockSpec(memory_space=pltpu.VMEM)
    anyspec = pl.BlockSpec(memory_space=pl.ANY)
    smem = pl.BlockSpec(memory_space=pltpu.SMEM)
    big = (4, 128, 2048)
    rows4 = (4, 64, 2048)
    dma = pltpu.SemaphoreType.DMA
    return pl.pallas_call(
        layer_kernel,
        out_shape=jax.ShapeDtypeStruct((256, 2048), BF),
        in_specs=[vm, vm, vm, vm, smem, vm, vm, vm] + [anyspec] * 5,
        out_specs=vm,
        scratch_shapes=[
            pltpu.VMEM((2, 1280, 128), BF),
            pltpu.VMEM((2, 1280, 256), BF),
            pltpu.VMEM((10, 1, 128), jnp.int32),
            pltpu.VMEM((2, 128, 128), BF),
            pltpu.VMEM((2, 128, 128), BF),
            pltpu.VMEM((3, 256, 512), BF),
            pltpu.VMEM((4, 256, 512), BF),
            pltpu.VMEM((3, 512, 2048), BF),
            pltpu.VMEM((512, 2048), BF),
            pltpu.VMEM((256, 2048), BF),
            pltpu.VMEM((256, 2048), F32),
            pltpu.VMEM((128, 384), F32),
            pltpu.VMEM((2, 512, 384), F32),
            pltpu.VMEM((2, 512, 384), BF),
            pltpu.VMEM((256, 128), F32),
            pltpu.VMEM((256, 2048), BF),
            pltpu.VMEM(rows4, BF),
            pltpu.VMEM((8, 64, 2048), BF),
            pltpu.VMEM((4, 8, 128), F32),
            pltpu.VMEM((8, 8, 128), F32),
            pltpu.VMEM((16, 256), F32),
            pltpu.VMEM((256, 256), BF),
            pltpu.VMEM((256, 256), BF),
            pltpu.VMEM((4, 128, 128), BF),
            pltpu.VMEM((4, 128, 128), BF),
            pltpu.VMEM(big, BF),
            pltpu.VMEM(big, BF),
            pltpu.VMEM(big, BF),
            pltpu.VMEM(big, BF),
            pltpu.VMEM(rows4, F32),
            pltpu.VMEM(rows4, BF),
            pltpu.VMEM(rows4, BF),
            pltpu.VMEM((3, 64, 2048), BF),
            pltpu.VMEM(rows4, BF),
            pltpu.VMEM(rows4, BF),
            pltpu.VMEM((2048, 512), BF),
            pltpu.VMEM((2048, 512), BF),
            pltpu.VMEM((512, 2048), BF),
            dma((84,)), dma((84,)), dma((74,)), dma((74,)), dma((5,)),
        ],
        compiler_params=pltpu.CompilerParams(
            collective_id=0, has_side_effects=True, vmem_limit_bytes=62 * 2**20
        ),
        name="layer",
    )(
        queries, key_rows, value_rows, doc_ids.reshape(8, 1, 128), sink_logit,
        norm_gain.reshape(1, 2048), routes.T, route_weights.T, residual, out_weight,
        gate_weight, up_weight, down_weight,
    )


def per_device(
    queries,
    key_rows,
    value_rows,
    doc_ids,
    sink_logit,
    residual,
    out_weight,
    norm_gain,
    gate_weight,
    up_weight,
    down_weight,
    routes,
    route_weights,
):
    return layer(
        queries, key_rows, value_rows, doc_ids, sink_logit, residual, out_weight, norm_gain,
        gate_weight, up_weight, down_weight, routes, route_weights,
    )


def solution(mesh):
    return jax.shard_map(
        per_device,
        mesh=mesh,
        in_specs=(
            P("sp", "tp"),
            P("sp", "tp"),
            P("sp", "tp"),
            P("sp"),
            P("tp"),
            P(("sp", "tp"), None),
            P("tp", None),
            P(),
            P("sp", None, None),
            P("sp", None, None),
            P("sp", None, None),
            P(("sp", "tp"), None),
            P(("sp", "tp"), None),
        ),
        out_specs=P(("sp", "tp"), None),
        check_vma=False,
    )
```
